32 devices in a mesh: ep: 8 (over z, core), tp: 4 (over y, x).
Axes of the slice: x: 2, y: 2, z: 4, core: 2. Of those that a mesh axis runs over, the one named last changes fastest.
Arguments:
- tokens: bfloat16 [1024, 2048], P('ep', 'tp'), may hold values from -6 to 6
- routing: int32 [1024, 2], P('ep'), may hold values from 0 to 3, all different within a row; in each aligned block of 128 rows (0 to 127, 128 to 255, ...) at most 80 rows name the same one
- mixing: float32 [1024, 2], P('ep'), may hold values from 0.1 to 0.9
- gate_matrix: bfloat16 [8, 2048, 2048], P('ep', None, 'tp'), may hold values from -0.125 to 0.125
- up_matrix: bfloat16 [8, 2048, 2048], P('ep', None, 'tp'), may hold values from -0.125 to 0.125
- down_matrix: bfloat16 [8, 2048, 2048], P('ep', 'tp'), may hold values from -0.09375 to 0.09375
- upstream: bfloat16 [1024, 2048], P('ep', 'tp'), may hold values from -6 to 6
Outputs:
- token_gradient: bfloat16 [1024, 2048], P('ep', 'tp')
- mixing_gradient: float32 [1024, 2], P('ep')
- gate_gradient: bfloat16 [8, 2048, 2048], P('ep', None, 'tp')
- up_gradient: bfloat16 [8, 2048, 2048], P('ep', None, 'tp')
- down_gradient: bfloat16 [8, 2048, 2048], P('ep', 'tp')
- input_norms: float32 [8, 2, 2048], P('ep')
- down_norms: float32 [8, 2048], P('ep', 'tp')
The draws below stay inside these ranges and needn't reach their ends.
Inputs may be any that keep to these rules, and one draw needn't show every extreme that they name: `routing`: A token's 2 experts differ. In each aligned block of 128 rows (the rows of one index of ep) no expert is named by more than 80 rows, and in every draw some expert is named by exactly 80 rows of some block.
All inputs are finite; a program needn't handle non-finite values.
Results may differ from the reference program's by a relative error of at most 0.0064.
Values may be sent and summed in bfloat16 or wider, within the bound.
A program may use at most 64 MiB of HBM per device.

```python
import math
from functools import partial
import jax
import jax.numpy as jnp
import numpy as np
from jax import lax

D = 2048
FF = 4096
TOP = 2
TOK_DEV = 128
EXPERTS = 4
SLABS = 8
FF_HALF = 2048
CAP = 80
TOKENS = 1024
N_EP = 8
N_TP = 4


def levels(rng, extent, pieces, least, high):
    loudness = 1.0
    for axis_at, blocks in pieces:
        steps = jax.random.uniform(jax.random.fold_in(jax.random.fold_in(rng, 6), axis_at), (blocks,), jnp.float32, least / len(pieces), high / len(pieces))
        loudness = loudness * jnp.repeat(jnp.exp(steps), extent[axis_at] // blocks).reshape((-1,) + (1,) * (len(extent) - 1 - axis_at))
    return loudness


def routed_block(own_key, own, number, rows, count, top, bound, lean):
    ranking = jax.random.permutation(own_key, count)
    packed, common = shares(count, rows * top, bound, lean, True), shares(count, rows * top, bound, lean, False)
    places = jnp.arange(count)

    def named(lengths, turn):
        used = int((lengths > 0).sum())
        fixed = max(1, used // 4)
        shifted = fixed + (places - fixed + turn * (used - fixed)) % max(1, count - fixed)
        return jnp.zeros((count,), jnp.int32).at[ranking[jnp.where(places < fixed, places, shifted)]].set(jnp.asarray(lengths, jnp.int32))

    lengths = jnp.where(number % 4 == 0, named(packed, number // 4), named(common, number - number // 4 - 1))
    mixed = jax.random.permutation(jax.random.fold_in(own, 3), count)
    source_of, receiver = mixed[0:count // 2 * 2:2], mixed[1:count // 2 * 2:2]
    slack = jnp.minimum(lengths[source_of] - 1, bound - lengths[receiver]) // 2
    slack = jnp.where((source_of == ranking[0]) | (receiver == ranking[0]) | (lengths[receiver] == 0), 0, jnp.maximum(slack, 0))
    shifted = jax.random.randint(jax.random.fold_in(own, 4), (count // 2,), 0, 1 << 20) % (slack + 1)
    lengths = lengths.at[source_of].add(-shifted).at[receiver].add(shifted)
    members = jnp.searchsorted(jnp.cumsum(lengths), jnp.arange(rows * top), side="right").astype(jnp.int32)
    listing = members.reshape(top, rows).T
    listing = listing[jax.random.permutation(jax.random.fold_in(own, 1), rows)]
    turn = jax.random.randint(jax.random.fold_in(own, 2), (rows, 1), 0, top)
    return jnp.take_along_axis(listing, (jnp.arange(top)[None, :] + turn) % top, axis=1)


def shares(amount, total, most, skew, full):
    loads = [(1 << 20) // math.isqrt(rank ** skew) + 1 for rank in range(1, amount + 1)]
    largest = most if full else min(most, max(-(-total // amount), total * loads[0] // sum(loads)))
    least = 1 if total - largest >= amount - 1 else 0
    given, spare = [largest] + [least] * (amount - 1), total - largest - least * (amount - 1)
    while spare > 0:
        candidates = [i for i in range(1, amount) if given[i] < largest] or [i for i in range(1, amount) if given[i] < most]
        whole, budget = sum([loads[i] for i in candidates]), spare
        for i in candidates:
            addition = min(most - given[i], max(1, budget * loads[i] // whole), spare)
            given[i] = given[i] + addition
            spare = spare - addition
    return np.array(given)


def noise(own_key, extent, width, most, cuts=(), held_as=jnp.bfloat16):
    result = jax.random.normal(own_key, extent, jnp.float32) * width
    if len(cuts) > 0:
        result = levels(own_key, extent, cuts, -0.22, 0.18) * result
    return jnp.clip(result, min=-most, max=most).astype(held_as)


def setup_inputs(seed: int = 0) -> dict:
    key_list = jax.random.split(jax.random.key(seed), 8)
    tokens = noise(key_list[0], (TOKENS, D), 1.0, 6.0, ((0, 8), (1, 4)))
    routing_keys = jax.random.split(jax.random.fold_in(key_list[1], 1), TOKENS // TOK_DEV)
    routing_turns = jax.random.permutation(jax.random.fold_in(key_list[1], 3), TOKENS // TOK_DEV)
    routing = jax.vmap(lambda own, number: routed_block(jax.random.fold_in(key_list[1], 2), own, number, TOK_DEV, EXPERTS, TOP, CAP, 1))(routing_keys, routing_turns).reshape((TOKENS, TOP))
    mixing = jnp.clip(0.1 + 0.79999997 * jax.random.uniform(key_list[2], (TOKENS, TOP), jnp.float32) ** levels(key_list[2], (TOKENS, TOP), ((0, 8),), -0.2, 0.2), 0.1, 0.9)
    gate_matrix = noise(key_list[3], (SLABS, D, FF_HALF), D ** -0.5, 0.125, ((0, 8), (2, 4)))
    up_matrix = noise(key_list[4], (SLABS, D, FF_HALF), D ** -0.5, 0.125, ((0, 8), (2, 4)))
    down_matrix = noise(key_list[5], (SLABS, FF_HALF, D), FF ** -0.5, 0.09375, ((0, 8), (1, 4)))
    upstream = noise(key_list[6], (TOKENS, D), 1.0, 6.0, ((0, 8), (1, 4)))
    return dict(tokens=tokens, routing=routing, mixing=mixing, gate_matrix=gate_matrix, up_matrix=up_matrix, down_matrix=down_matrix, upstream=upstream)


def slot_targets(route_block, experts, capacity):
    flat_routes = route_block.reshape(-1).astype(jnp.int32)
    choose = (flat_routes[:, None] == jnp.arange(experts, dtype=jnp.int32)[None, :]).astype(jnp.int32)
    earlier = jnp.cumsum(choose, axis=0) - choose
    return (flat_routes * capacity + jnp.sum(earlier * choose, axis=1)).astype(jnp.int32)


def place_rows(target, values, slot_count):
    matches = (target[:, None] == jnp.arange(slot_count, dtype=jnp.int32)[None, :]).astype(values.dtype)
    placed = lax.dot_general(matches, values, (((0,), (0,)), ((), ())), preferred_element_type=jnp.float32)
    return placed.astype(jnp.bfloat16)


def take_rows(values, target):
    return jnp.take(values, target, axis=0)


def expert_backward(token_rows, grad_rows, gate_mat, up_mat, down_mat):
    gate_pre = jnp.dot(token_rows, gate_mat, preferred_element_type=jnp.float32)
    up_pre = jnp.dot(token_rows, up_mat, preferred_element_type=jnp.float32)
    sigmoid_gate = jax.nn.sigmoid(gate_pre)
    activated = gate_pre * sigmoid_gate
    hidden = activated * up_pre
    back_grad = lax.dot_general(grad_rows, down_mat, (((1,), (1,)), ((), ())), preferred_element_type=jnp.float32)
    up_grad = (back_grad * activated).astype(jnp.bfloat16)
    gate_grad = (back_grad * up_pre * sigmoid_gate * (1.0 + gate_pre * (1.0 - sigmoid_gate))).astype(jnp.bfloat16)
    hidden_low = hidden.astype(jnp.bfloat16)
    contract_rows = (((0,), (0,)), ((), ()))
    down_full = lax.dot_general(hidden_low, grad_rows, contract_rows, preferred_element_type=jnp.float32)
    gate_full = lax.dot_general(token_rows, gate_grad, contract_rows, preferred_element_type=jnp.float32)
    up_full = lax.dot_general(token_rows, up_grad, contract_rows, preferred_element_type=jnp.float32)
    scores = jnp.sum(hidden * back_grad, axis=1)
    return gate_full, up_full, down_full, gate_grad, up_grad, scores


def reference(tokens, routing, mixing, gate_matrix, up_matrix, down_matrix, upstream):
    sources = N_EP
    slot_count = EXPERTS * CAP
    route_blocks = routing.reshape(sources, TOK_DEV, TOP)
    targets = jax.vmap(partial(slot_targets, experts=EXPERTS, capacity=CAP))(route_blocks)
    scaled = (mixing[:, :, None] * upstream[:, None, :].astype(jnp.float32)).astype(jnp.bfloat16)
    spread_tokens = jnp.repeat(tokens.reshape(sources, TOK_DEV, D), TOP, axis=1)
    spread_grads = scaled.reshape(sources, TOK_DEV * TOP, D)
    placing = jax.vmap(partial(place_rows, slot_count=slot_count))

    def to_experts(placed):
        return placed.reshape(sources, EXPERTS, CAP, D).transpose(1, 0, 2, 3).reshape(EXPERTS, sources * CAP, D)

    expert_tokens = to_experts(placing(targets, spread_tokens))
    expert_grads = to_experts(placing(targets, spread_grads))
    gate_whole = gate_matrix.reshape(EXPERTS, 2, D, FF_HALF).transpose(0, 2, 1, 3).reshape(EXPERTS, D, FF)
    up_whole = up_matrix.reshape(EXPERTS, 2, D, FF_HALF).transpose(0, 2, 1, 3).reshape(EXPERTS, D, FF)
    down_whole = down_matrix.reshape(EXPERTS, FF, D)

    def one_expert(inputs):
        token_rows, grad_rows, gate_mat, up_mat, down_mat = inputs
        gate_full, up_full, down_full, gate_grad, up_grad, scores = expert_backward(token_rows, grad_rows, gate_mat, up_mat, down_mat)
        blocks = 2 * N_TP
        block_width = FF // blocks

        def add_block(block_index, running):
            start = (block_index * block_width).astype(jnp.int32)
            gate_piece = lax.dynamic_slice_in_dim(gate_grad, start, block_width, 1)
            up_piece = lax.dynamic_slice_in_dim(up_grad, start, block_width, 1)
            gate_cols = lax.dynamic_slice_in_dim(gate_mat, start, block_width, 1)
            up_cols = lax.dynamic_slice_in_dim(up_mat, start, block_width, 1)
            contract_cols = (((1,), (1,)), ((), ()))
            block_term = lax.dot_general(gate_piece, gate_cols, contract_cols, preferred_element_type=jnp.float32)
            block_term = block_term + lax.dot_general(up_piece, up_cols, contract_cols, preferred_element_type=jnp.float32)
            rounded = lax.optimization_barrier(block_term.astype(jnp.bfloat16))
            return running + rounded.astype(jnp.float32)

        pair_grad = lax.fori_loop(0, blocks, add_block, jnp.zeros((token_rows.shape[0], D), jnp.float32))
        gate_norm = jnp.sum(jnp.square(gate_full).reshape(D, 2, FF_HALF), axis=2).T
        up_norm = jnp.sum(jnp.square(up_full).reshape(D, 2, FF_HALF), axis=2).T
        input_norm = jnp.stack([gate_norm, up_norm], axis=1)
        down_norm = jnp.sum(down_full * down_full, axis=1)
        return (gate_full.astype(jnp.bfloat16), up_full.astype(jnp.bfloat16), down_full.astype(jnp.bfloat16),
                input_norm, down_norm, pair_grad, scores)

    results = lax.map(one_expert, (expert_tokens, expert_grads, gate_whole, up_whole, down_whole))
    gate_out, up_out, down_out, input_norm, down_norm, pair_grad, scores = results
    gate_gradient = gate_out.reshape(EXPERTS, D, 2, FF_HALF).transpose(0, 2, 1, 3).reshape(SLABS, D, FF_HALF)
    up_gradient = up_out.reshape(EXPERTS, D, 2, FF_HALF).transpose(0, 2, 1, 3).reshape(SLABS, D, FF_HALF)
    down_gradient = down_out.reshape(SLABS, FF_HALF, D)
    input_norms = input_norm.reshape(SLABS, 2, D)
    down_norms = down_norm.reshape(SLABS, FF_HALF)
    back_rows = pair_grad.reshape(EXPERTS, sources, CAP, D).transpose(1, 0, 2, 3).reshape(sources, slot_count, D)
    gathered_rows = jax.vmap(take_rows)(back_rows, targets)
    token_gradient = jnp.sum(gathered_rows.reshape(TOKENS, TOP, D), axis=1).astype(jnp.bfloat16)
    back_scores = scores.reshape(EXPERTS, sources, CAP).transpose(1, 0, 2).reshape(sources, slot_count)
    mixing_gradient = jax.vmap(take_rows)(back_scores, targets).reshape(TOKENS, TOP) / mixing
    return (token_gradient, mixing_gradient, gate_gradient, up_gradient, down_gradient, input_norms, down_norms)
```

```python
import functools

import jax
import jax.numpy as jnp
from jax import lax
from jax.experimental import pallas as pl
from jax.experimental.pallas import tpu as pltpu
from jax.sharding import PartitionSpec as P

MESH = pl.DeviceIdType.MESH
F32 = jnp.float32
BF16 = jnp.bfloat16


def send(src, dst, send_sem, recv_sem, ep, tp):
    copy = pltpu.make_async_remote_copy(
        src_ref=src, dst_ref=dst, send_sem=send_sem, recv_sem=recv_sem,
        device_id=(ep, tp), device_id_type=MESH,
    )
    copy.start()
    return copy


def arrived(ref, sem):
    pltpu.make_async_copy(ref, ref, sem).wait()


def places():
    ep, tp = lax.axis_index("ep"), lax.axis_index("tp")
    return ep // 2, ep % 2, tp


def tp_peer(tp, step, n_tp):
    if n_tp == 4:
        x, y = tp % 2, tp // 2
        return ((1 - y) if step // 2 else y) * 2 + ((1 - x) if step % 2 else x)
    return (tp + step) % n_tp


def tp_from(tp, step, n_tp):
    if n_tp == 4:
        return tp_peer(tp, step, n_tp)
    return (tp + n_tp - step) % n_tp


def greet(zs, n_tp, z, c, t):
    barrier = pltpu.get_barrier_semaphore()
    for k in range(1, zs):
        pl.semaphore_signal(barrier, inc=1, device_id=((z + k) % zs * 2 + c, t), device_id_type=MESH)
    for k in range(1, n_tp):
        pl.semaphore_signal(barrier, inc=1, device_id=(z * 2 + c, (t + k) % n_tp), device_id_type=MESH)
    pl.semaphore_signal(barrier, inc=1, device_id=(z * 2 + 1 - c, t), device_id_type=MESH)
    pl.semaphore_wait(barrier, zs + n_tp - 1)


def distances(zs):
    order = []
    for k in range(1, zs // 2 + 1):
        order.append(k)
        if zs - k != k:
            order.append(zs - k)
    return order


def dispatch_kernel(
    zs, n_tp, part, x_in, y_in, x_out, y_out, ep_send, ep_recv, tp_send, tp_recv,
    fwd_send, core_send, core_recv,
):
    z, c, t = places()
    chunks = zs if zs <= 4 else 1
    span = zs // chunks
    ins, outs = (x_in, y_in), (x_out, y_out)
    greet(zs, n_tp, z, c, t)

    def block(a, core, q, feat):
        cols = pl.ds(pl.multiple_of(feat * part, part), part)
        return outs[a].at[core, pl.ds(q * span, span), :, cols]

    def mine(a):
        cols = pl.ds(pl.multiple_of(t * part, part), part)
        return outs[a].at[c, z, :, cols]

    sent = []
    home = z // span
    for a in range(2):
        pltpu.make_async_copy(ins[a].at[z], mine(a), ep_recv.at[a, home]).start()
    for k in distances(zs):
        for a in range(2):
            dest = (z + k) % zs
            sent.append(send(ins[a].at[dest], mine(a), ep_send.at[a, k], ep_recv.at[a, home], dest * 2 + c, t))

    direct = (1, 2) if n_tp == 4 else range(1, n_tp)

    def to_core(a, q, feat):
        ref = block(a, c, q, feat)
        sent.append(send(ref, ref, core_send.at[a, q, feat], core_recv.at[a, q, feat], z * 2 + 1 - c, t))

    def spread(q):
        for a in range(2):
            ref = block(a, c, q, t)
            arrived(ref, ep_recv.at[a, q])
            for s in direct:
                sent.append(send(ref, ref, tp_send.at[a, q, s], tp_recv.at[a, q, t], z * 2 + c, tp_peer(t, s, n_tp)))
            to_core(a, q, t)

    def relay(q):
        if n_tp == 4:
            for a, s in ((0, 1), (1, 2), (1, 1), (0, 2)):
                feat = tp_from(t, s, n_tp)
                ref = block(a, c, q, feat)
                arrived(ref, tp_recv.at[a, q, feat])
                if s == a + 1:
                    sent.append(send(ref, ref, fwd_send.at[a, q], tp_recv.at[a, q, feat], z * 2 + c, tp_peer(t, 3 - s, n_tp)))
                to_core(a, q, feat)
        else:
            for s in direct:
                feat = tp_from(t, s, n_tp)
                for a in range(2):
                    arrived(block(a, c, q, feat), tp_recv.at[a, q, feat])
                    to_core(a, q, feat)

    def finish(q):
        if n_tp == 4:
            feat = tp_from(t, 3, n_tp)
            for a in range(2):
                arrived(block(a, c, q, feat), tp_recv.at[a, q, feat])
                to_core(a, q, feat)

    if chunks == 1:
        order = [0]
    else:
        order = [z] + [(z + zs - k) % zs for k in distances(zs)]
    for i in range(chunks + 2):
        if i < chunks:
            spread(order[i])
        if 1 <= i <= chunks:
            relay(order[i - 1])
        if i >= 2:
            finish(order[i - 2])
    for a in range(2):
        for q in range(chunks):
            for feat in range(n_tp):
                arrived(block(a, 1 - c, q, feat), core_recv.at[a, q, feat])
    for copy in sent:
        copy.wait_send()


def dispatch(x, y, zs, n_tp):
    _, cap, part = x.shape
    chunks = zs if zs <= 4 else 1
    out = jax.ShapeDtypeStruct((2, zs, cap, n_tp * part), BF16)
    vm = pl.BlockSpec(memory_space=pltpu.VMEM)
    dma = pltpu.SemaphoreType.DMA
    return pl.pallas_call(
        functools.partial(dispatch_kernel, zs, n_tp, part),
        out_shape=(out, out),
        in_specs=[vm, vm],
        out_specs=(vm, vm),
        scratch_shapes=[
            dma((2, zs)), dma((2, chunks)), dma((2, chunks, n_tp)), dma((2, chunks, n_tp)),
            dma((2, chunks)), dma((2, chunks, n_tp)), dma((2, chunks, n_tp)),
        ],
        compiler_params=pltpu.CompilerParams(collective_id=0, has_side_effects=True, vmem_limit_bytes=48 << 20),
        name="dispatch",
    )(x, y)


def hail(zs, n_tp, z, c, t):
    barrier = pltpu.get_barrier_semaphore()
    for k in range(1, zs):
        pl.semaphore_signal(barrier, inc=1, device_id=((z + k) % zs * 2 + c, t), device_id_type=MESH)
    for k in range(1, n_tp):
        pl.semaphore_signal(barrier, inc=1, device_id=(z * 2 + c, (t + k) % n_tp), device_id_type=MESH)
    pl.semaphore_signal(barrier, inc=1, device_id=(z * 2 + 1 - c, t), device_id_type=MESH)
    return lambda: pl.semaphore_wait(barrier, zs + n_tp - 1)


def lane_sums(square):
    folded = square[:, :128]
    for k in range(1, square.shape[1] // 128):
        folded = folded + square[:, k * 128:(k + 1) * 128]
    return jnp.sum(folded.T, axis=0, keepdims=True)


def return_kernel(
    zs, n_tp, part,
    gate_hbm, up_hbm, w_gate_hbm, w_up_hbm, x_hbm, hidden_hbm, y_hbm, scores,
    out_rows, out_scores, out_norms, out_down_norms, gate_out, up_out, down_out,
    gate_grad, up_grad, w_gate, w_up, x, hidden, y, gate_full, up_full, down_full, norms, folded,
    all_rows, other, other_scores, both, both_scores, pieces, score_pieces, norm_pieces, total, total_scores,
    passing, passed, pass_send, pass_recv, sum_send, sum_recv, load_sem, store_sem,
    core_send, core_recv, cs_send, cs_recv, tp_send, tp_recv, ts_send, ts_recv,
    tn_send, tn_recv, ep_send, ep_recv, es_send, es_recv,
):
    z, c, t = places()
    chunks = zs if zs <= 4 else 1
    span = zs // chunks
    cap = out_rows.shape[1]
    width, hid = w_gate.shape
    half = zs * cap
    everyone_in = hail(zs, n_tp, z, c, t)
    loads = []
    for i, (src, dst) in enumerate((
        (gate_hbm, gate_grad), (up_hbm, up_grad), (w_gate_hbm, w_gate), (w_up_hbm, w_up),
        (x_hbm, x), (hidden_hbm, hidden), (y_hbm, y),
    )):
        copy = pltpu.make_async_copy(src, dst, load_sem.at[i])
        copy.start()
        loads.append(copy)
    stores = []

    def store(i, src, dst):
        copy = pltpu.make_async_copy(src, dst, store_sem.at[i])
        copy.start()
        stores.append(copy)

    across = (((1,), (1,)), ((), ()))
    down = (((0,), (0,)), ((), ()))
    tile = min(256, width)

    def row_terms():
        @pl.loop(0, width // tile)
        def _(j):
            at = pl.ds(pl.multiple_of(j * tile, tile), tile)
            term = (
                lax.dot_general(gate_grad[...].reshape(2 * half, hid), w_gate[at, :], across, preferred_element_type=F32)
                + lax.dot_general(up_grad[...].reshape(2 * half, hid), w_up[at, :], across, preferred_element_type=F32)
            ).astype(BF16)
            all_rows[0, :, at] = term[:half]
            all_rows[1, :, at] = term[half:]

    sent = []
    if chunks == 1:
        order = [0]
    else:
        order = [(z + k) % zs for k in reversed(distances(zs))] + [z]
    mate = z * 2 + 1 - c

    def rows_of(q):
        if chunks == 1:
            return slice(None)
        return pl.ds(pl.multiple_of(q * cap, cap), cap)

    for copy in loads[:4]:
        copy.wait()
    row_terms()
    everyone_in()
    for q in order:
        sent.append(send(all_rows.at[1 - c, rows_of(q)], other.at[rows_of(q)], core_send.at[q], core_recv.at[q], mate, t))
    sent.append(send(scores.at[1 - c], other_scores, cs_send, cs_recv, mate, t))

    def cols(feat):
        return pl.ds(pl.multiple_of(feat * part, part), part)

    def reduce_core(q):
        at = rows_of(q)
        arrived(other.at[at], core_recv.at[q])
        both[at, :] = (all_rows[c, at, :].astype(F32) + other[at, :].astype(F32)).astype(BF16)
        if n_tp == 4:
            far_side = tp_peer(t, 3, n_tp)
            for s in (1, 2):
                sent.append(send(both.at[at, half_cols(far_side, s - 1)], passing.at[s - 1, at], pass_send.at[s - 1, q], pass_recv.at[s - 1, q], z * 2 + c, tp_peer(t, s, n_tp)))
            for s in (1, 2):
                feat = tp_peer(t, s, n_tp)
                sent.append(send(both.at[at, half_cols(feat, s - 1)], piece_half(s, at, s - 1), tp_send.at[s, q], tp_recv.at[s, q], z * 2 + c, feat))
        else:
            for s in reversed(range(1, n_tp)):
                feat = tp_peer(t, s, n_tp)
                sent.append(send(both.at[at, cols(feat)], pieces.at[s, at], tp_send.at[s, q], tp_recv.at[s, q], z * 2 + c, feat))

    def half_cols(feat, u):
        return pl.ds(pl.multiple_of(feat * part + u * (part // 2), part // 2), part // 2)

    def piece_half(s, at, u):
        return pieces.at[s, at, pl.ds(u * (part // 2), part // 2)]

    def pass_on(q):
        if n_tp == 4:
            at = rows_of(q)
            for s in (1, 2):
                u, turn = s - 1, 3 - s
                feat = tp_peer(t, turn, n_tp)
                arrived(passing.at[u, at], pass_recv.at[u, q])
                passed[u, at, :] = (passing[u, at, :].astype(F32) + both[at, half_cols(feat, u)].astype(F32)).astype(BF16)
                sent.append(send(passed.at[u, at], piece_half(turn, at, u), sum_send.at[turn, q], sum_recv.at[turn, q], z * 2 + c, feat))

    for q in order:
        reduce_core(q)
    arrived(other_scores, cs_recv)
    both_scores[...] = scores[c] + other_scores[...]
    for s in range(1, n_tp):
        sent.append(send(both_scores, score_pieces.at[s], ts_send.at[s], ts_recv.at[s], z * 2 + c, tp_peer(t, s, n_tp)))

    def reduce_tp(q):
        at = rows_of(q)
        if n_tp == 4:
            for s in (1, 2):
                arrived(piece_half(s, at, s - 1), tp_recv.at[s, q])
                arrived(piece_half(s, at, 2 - s), sum_recv.at[s, q])
        else:
            for s in reversed(range(1, n_tp)):
                arrived(pieces.at[s, at], tp_recv.at[s, q])
        for j in range(span):
            sub = at if chunks > 1 else slice(j * cap, (j + 1) * cap)
            acc = both[sub, cols(t)].astype(F32)
            for s in (1, 2) if n_tp == 4 else range(1, n_tp):
                acc = acc + pieces[s, sub, :].astype(F32)
            total[q * span + j] = acc.astype(BF16)

    def go_home(dest, k):
        sent.append(send(total.at[dest], out_rows.at[z], ep_send.at[k], ep_recv.at[k], dest * 2 + c, t))

    def input_tiles(first, last):
        @pl.loop(first * tile // g_tile, last * tile // g_tile)
        def _(j):
            at = pl.ds(pl.multiple_of(j * g_tile, g_tile), g_tile)
            columns = x[:, at].T
            for i, (grad, full) in enumerate(((gate_grad, gate_full), (up_grad, up_full))):
                term = jnp.dot(columns, grad[...].reshape(2 * half, hid), preferred_element_type=F32)
                full[at, :] = term.astype(BF16)
                norms[pl.ds(i, 1), at] = lane_sums(term * term)

    h_tile = min(256, hid)
    g_tile = min(512, width)
    wide = min(512, width)

    def down_tiles(i):
        at = slice(i * h_tile, (i + 1) * h_tile)
        folded[...] = jnp.zeros_like(folded)
        turned = hidden[:, at].T

        @pl.loop(0, width // wide)
        def _(j):
            lanes = pl.ds(pl.multiple_of(j * wide, wide), wide)
            term = jnp.dot(turned, y[:, lanes], preferred_element_type=F32)
            down_full[at, lanes] = term.astype(BF16)
            square = term * term
            acc = square[:, :128]
            for k in range(1, wide // 128):
                acc = acc + square[:, k * 128:(k + 1) * 128]
            folded[...] += acc

        out_down_norms[:, at] = jnp.sum(folded[...].T, axis=0, keepdims=True)

    away = list(reversed(distances(zs)))
    n_tiles = width // tile

    def phase_input(first, last):
        if first == 0:
            loads[4].wait()
        input_tiles(first, last)
        if last == n_tiles:
            store(0, gate_full, gate_out)
            store(1, up_full, up_out)
            for s in range(1, n_tp):
                sent.append(send(norms, norm_pieces.at[s], tn_send.at[s], tn_recv.at[s], z * 2 + c, tp_peer(t, s, n_tp)))

    def phase_down(first, last):
        if first == 0:
            loads[5].wait()
            loads[6].wait()
        for i in range(first, last):
            down_tiles(i)
        if last == hid // h_tile:
            store(2, down_full, down_out)

    h_count = hid // h_tile
    phases = [
        lambda: phase_input(0, n_tiles // 2),
        lambda: phase_input(n_tiles // 2, n_tiles),
        lambda: phase_down(0, h_count // 2) if h_count > 1 else None,
        lambda: phase_down(h_count // 2, h_count),
    ]
    if chunks < len(phases):
        for phase in phases:
            phase()
        phases = []
    pass_on(order[0])
    if chunks > 1:
        pass_on(order[1])
    for i in range(chunks):
        if i < len(phases):
            phases[i]()
        if i + 2 < chunks:
            pass_on(order[i + 2])
        reduce_tp(order[i])
        if chunks > 1:
            if i < len(away):
                go_home(order[i], away[i])
        else:
            for k in away:
                go_home((z + k) % zs, k)
        if i == 0:
            for s in range(1, n_tp):
                arrived(score_pieces.at[s], ts_recv.at[s])
            acc = both_scores[...]
            for s in range(1, n_tp):
                acc = acc + score_pieces[s]
            total_scores[...] = acc
            for k in away:
                dest = (z + k) % zs
                sent.append(send(total_scores.at[dest], out_scores.at[z], es_send.at[k], es_recv.at[k], dest * 2 + c, t))
            out_scores[z] = total_scores[z]
    out_rows[z] = total[z]
    acc = norms[...]
    for s in range(1, n_tp):
        arrived(norm_pieces.at[s], tn_recv.at[s])
        acc = acc + norm_pieces[s]
    out_norms[...] = acc
    for k in away:
        src = (z + zs - k) % zs
        arrived(out_scores.at[src], es_recv.at[k])
        arrived(out_rows.at[src], ep_recv.at[k])
    for copy in stores:
        copy.wait()
    for copy in sent:
        copy.wait_send()


def send_back(gate_grad, up_grad, w_gate, w_up, x, hidden, y, scores, zs, n_tp):
    rows, width = x.shape
    hid = hidden.shape[1]
    part, half = width // n_tp, rows // 2
    cap = half // zs
    chunks = zs if zs <= 4 else 1
    vm = pl.BlockSpec(memory_space=pltpu.VMEM)
    far = pl.BlockSpec(memory_space=pltpu.HBM)
    dma = pltpu.SemaphoreType.DMA
    line = scores.shape[2:]
    gradient = jax.ShapeDtypeStruct((width, hid), BF16)
    return pl.pallas_call(
        functools.partial(return_kernel, zs, n_tp, part),
        out_shape=(
            jax.ShapeDtypeStruct((zs, cap, part), BF16),
            jax.ShapeDtypeStruct((zs,) + line, F32),
            jax.ShapeDtypeStruct((2, width), F32),
            jax.ShapeDtypeStruct((1, hid), F32),
            gradient, gradient, jax.ShapeDtypeStruct((hid, width), BF16),
        ),
        in_specs=[far] * 7 + [vm],
        out_specs=(vm,) * 4 + (far,) * 3,
        scratch_shapes=[
            pltpu.VMEM((2, half, hid), BF16), pltpu.VMEM((2, half, hid), BF16),
            pltpu.VMEM((width, hid), BF16), pltpu.VMEM((width, hid), BF16),
            pltpu.VMEM((rows, width), BF16), pltpu.VMEM((rows, hid), BF16), pltpu.VMEM((rows, width), BF16),
            pltpu.VMEM((width, hid), BF16), pltpu.VMEM((width, hid), BF16), pltpu.VMEM((hid, width), BF16),
            pltpu.VMEM((2, width), F32), pltpu.VMEM((min(256, hid), 128), F32),
            pltpu.VMEM((2, half, width), BF16), pltpu.VMEM((half, width), BF16),
            pltpu.VMEM((zs,) + line, F32),
            pltpu.VMEM((half, width), BF16),
            pltpu.VMEM((zs,) + line, F32),
            pltpu.VMEM((n_tp, half, part), BF16),
            pltpu.VMEM((n_tp, zs) + line, F32),
            pltpu.VMEM((n_tp, 2, width), F32),
            pltpu.VMEM((zs, cap, part), BF16),
            pltpu.VMEM((zs,) + line, F32),
            pltpu.VMEM((2, half, part // 2), BF16), pltpu.VMEM((2, half, part // 2), BF16),
            dma((2, chunks)), dma((2, chunks)), dma((3, chunks)), dma((3, chunks)),
            dma((7,)), dma((3,)),
            dma((chunks,)), dma((chunks,)), dma, dma,
            dma((n_tp, chunks)), dma((n_tp, chunks)), dma((n_tp,)), dma((n_tp,)),
            dma((n_tp,)), dma((n_tp,)), dma((zs,)), dma((zs,)), dma((zs,)), dma((zs,)),
        ],
        compiler_params=pltpu.CompilerParams(collective_id=1, has_side_effects=True, vmem_limit_bytes=50 << 20),
        name="send_back",
    )(gate_grad.reshape(2, half, hid), up_grad.reshape(2, half, hid), w_gate, w_up, x, hidden, y, scores)


def fused_kernel(
    zs, n_tp, part, cap, tok,
    routing_hbm, mixing_hbm, tokens_hbm, upstream_hbm, w_gate_hbm, w_up_hbm, w_down_hbm,
    tokens_out, mixing_out, norms_out, down_norms_out, gate_out, up_out, down_out,
    out_tokens, out_mixing, out_norms, out_down_norms, gate_full, up_full, down_full,
    routing, mixing, tokens, upstream, w_gate, w_up, w_down, gate_turned, up_turned, down_turned,
    x_put, y_put, x_all, y_all, gate_grad, up_grad, hidden, targets,
    all_rows, other, both, passing, passed, pieces, total, back_rows,
    scores, other_scores, both_scores, score_pieces, total_scores, back_scores,
    norms, norm_pieces,
    folded, load_sem, store_sem, own_sem, ep_send, ep_recv, tp_send, tp_recv, fwd_send, core_send, core_recv,
    swap_send, swap_recv, pass_send, pass_recv, half_send, half_recv, sum_send, sum_recv,
    cs_send, cs_recv, ts_send, ts_recv, tn_send, tn_recv, home_send, home_recv, es_send, es_recv,
):
    z, c, t = places()
    here, mate = z * 2 + c, z * 2 + 1 - c
    peers = [tp_peer(t, s, n_tp) for s in range(n_tp)]
    width, hid = w_gate.shape
    rows = 2 * cap
    everyone_in = hail(zs, n_tp, z, c, t)
    loads = []
    for i, (src, dst) in enumerate((
        (routing_hbm, routing), (mixing_hbm, mixing), (tokens_hbm, tokens), (upstream_hbm, upstream),
        (w_down_hbm, w_down), (w_gate_hbm, w_gate), (w_up_hbm, w_up),
    )):
        copy = pltpu.make_async_copy(src, dst, load_sem.at[i])
        copy.start()
        loads.append(copy)
    across = (((1,), (1,)), ((), ()))
    first = (((0,), (0,)), ((), ()))
    stores = []

    def store(i, src, dst):
        copy = pltpu.make_async_copy(src, dst, store_sem.at[i])
        copy.start()
        stores.append(copy)

    def push(src, dst, send_sem, recv_sem, ep, tp):
        send(src, dst, send_sem, recv_sem, ep, tp)

    def cols(feat):
        return pl.ds(pl.multiple_of(feat * part, part), part)

    def half_cols(feat, u):
        return pl.ds(pl.multiple_of(feat * part + u * (part // 2), part // 2), part // 2)

    lanes = -(-zs // 16) * 16
    experts_at = lax.broadcasted_iota(jnp.int32, (lanes, tok), 0)
    before = lax.broadcasted_iota(jnp.int32, (tok, tok), 0) < lax.broadcasted_iota(jnp.int32, (tok, tok), 1)
    for copy in loads[:2]:
        copy.wait()
    picks = [routing[k:k + 1, :] == experts_at for k in range(routing.shape[0])]
    chosen = sum(pick.astype(F32) for pick in picks)
    earlier = jnp.dot(chosen.astype(BF16), before.astype(F32).astype(BF16), preferred_element_type=F32)
    for k, pick in enumerate(picks):
        place = jnp.sum(jnp.where(pick, earlier, 0.0), axis=0, keepdims=True)
        targets[k:k + 1, :] = routing[k:k + 1, :] * cap + place.astype(jnp.int32)

    def matches(e):
        slots_at = lax.broadcasted_iota(jnp.int32, (cap, tok), 0) + e * cap
        return [targets[k:k + 1, :] == slots_at for k in range(len(picks))]

    for copy in loads[2:4]:
        copy.wait()
    for e in range(zs):
        hits = matches(e)
        pick = sum(hit.astype(F32) for hit in hits).astype(BF16)
        weight = sum(jnp.where(hit, mixing[k:k + 1, :], 0.0) for k, hit in enumerate(hits))
        x_put[e] = jnp.dot(pick, tokens[...], preferred_element_type=F32).astype(BF16)
        placed = jnp.dot(pick, upstream[...], preferred_element_type=F32)
        y_put[e] = (placed * jnp.sum(weight, axis=1, keepdims=True)).astype(BF16)
    scores[...] = jnp.zeros_like(scores)
    everyone_in()

    outer = (z - 1) * (z - 2) // 2
    order = [z, z + 1 - 2 * (z % 2), 2 - z // 2, 3 - 3 * (z // 2)]
    lands = [0, 1, 2 + outer, 2 + outer]
    puts, alls = (x_put, y_put), (x_all, y_all)

    def block(a, i, core, feat):
        return alls[a].at[i, core, :, cols(feat)]

    owns = []
    for a in range(2):
        copy = pltpu.make_async_copy(puts[a].at[z], block(a, 0, c, t), own_sem.at[a])
        copy.start()
        owns.append(copy)

    def over(i):
        return [
            pltpu.make_async_remote_copy(
                src_ref=puts[a].at[order[i]], dst_ref=block(a, lands[i], c, t), send_sem=ep_send.at[a],
                recv_sem=ep_recv.at[a, lands[i]], device_id=(order[i] * 2 + c, t), device_id_type=MESH,
            )
            for a in range(2)
        ]

    def cross(i):
        for copy in over(i):
            copy.start()

    def to_core(a, i, feat, src=None):
        ref = block(a, i, c, feat)
        push(ref if src is None else src, ref, core_send.at[a], core_recv.at[a, i, feat], mate, t)

    def spread(i):
        refs = [block(a, i, c, t) for a in range(2)]
        srcs = refs if i else [puts[a].at[z] for a in range(2)]
        if i:
            for a in range(2):
                arrived(refs[a], ep_recv.at[a, i])
        for a, s in ((0, 1), (1, 2), (1, 1), (0, 2)):
            push(srcs[a], refs[a], tp_send.at[a], tp_recv.at[a, i, t], here, peers[s])
        for a in range(2):
            to_core(a, i, t, srcs[a])

    def relay(i):
        for a, s in ((0, 1), (1, 2)):
            ref = block(a, i, c, peers[s])
            arrived(ref, tp_recv.at[a, i, peers[s]])
            push(ref, ref, fwd_send.at[a], tp_recv.at[a, i, peers[s]], here, peers[3 - s])
            to_core(a, i, peers[s])

    def finish(i):
        for a, s in ((1, 1), (0, 2), (0, 3), (1, 3)):
            arrived(block(a, i, c, peers[s]), tp_recv.at[a, i, peers[s]])
            to_core(a, i, peers[s])

    square = min(256, hid)
    eye = (
        lax.broadcasted_iota(jnp.int32, (square, square), 0) == lax.broadcasted_iota(jnp.int32, (square, square), 1)
    ).astype(F32).astype(BF16)

    def turn_down():
        loads[4].wait()

        @pl.loop(0, width // square, unroll=4)
        def _(j):
            at = pl.ds(pl.multiple_of(j * square, square), square)
            down_turned[at, :] = lax.dot_general(eye, w_down[:, at], across, preferred_element_type=F32).astype(BF16)

    def turn_in(a):
        loads[5 + a].wait()
        src, dst = ((w_gate, gate_turned), (w_up, up_turned))[a]

        @pl.loop(0, width // square, unroll=4)
        def _(j):
            at = pl.ds(pl.multiple_of(j * square, square), square)
            for h in range(hid // square):
                lines = slice(h * square, (h + 1) * square)
                dst[lines, at] = lax.dot_general(eye, src[at, lines], across, preferred_element_type=F32).astype(BF16)

    h_tile = min(256, hid)

    def forward(i):
        if i == 0:
            for copy in owns:
                copy.wait()
        for a in range(2):
            for feat in peers:
                arrived(block(a, i, 1 - c, feat), core_recv.at[a, i, feat])
        for j in range(hid // h_tile):
            at = slice(j * h_tile, (j + 1) * h_tile)
            gate_pre = jnp.dot(x_all[i].reshape(rows, width), w_gate[:, at], preferred_element_type=F32)
            up_pre = jnp.dot(x_all[i].reshape(rows, width), w_up[:, at], preferred_element_type=F32)
            back = jnp.dot(y_all[i].reshape(rows, width), down_turned[:, at], preferred_element_type=F32)
            sig = jax.nn.sigmoid(gate_pre)
            act = gate_pre * sig
            low = act * up_pre
            gate_grad[i, :, :, at] = (back * up_pre * sig * (1.0 + gate_pre * (1.0 - sig))).astype(BF16).reshape(2, cap, h_tile)
            up_grad[i, :, :, at] = (back * act).astype(BF16).reshape(2, cap, h_tile)
            hidden[i, :, :, at] = low.astype(BF16).reshape(2, cap, h_tile)
            terms = low * back
            for core in range(2):
                scores[core, i, :, :cap] += lane_sums(terms[core * cap:(core + 1) * cap])

    def row_terms(i):
        for s in (3, 1, 2, 0):
            at = cols(peers[s])
            term = (
                jnp.dot(gate_grad[i].reshape(rows, hid), gate_turned[:, at], preferred_element_type=F32)
                + jnp.dot(up_grad[i].reshape(rows, hid), up_turned[:, at], preferred_element_type=F32)
            ).astype(BF16)
            all_rows[i, :, :, at] = term.reshape(2, cap, part)
            push(all_rows.at[i, 1 - c, :, at], other.at[i, :, at], swap_send, swap_recv.at[i, s], mate, t)

    def piece_half(s, i, u):
        return pieces.at[s - 1, i, :, pl.ds(u * (part // 2), part // 2)]

    def reduce_core(i):
        for s in (3, 1, 2, 0):
            at = cols(peers[s])
            arrived(other.at[i, :, at], swap_recv.at[i, s])
            both[i, :, at] = (all_rows[i, c, :, at].astype(F32) + other[i, :, at].astype(F32)).astype(BF16)
            if s == 3:
                for u in range(2):
                    push(both.at[i, :, half_cols(peers[3], u)], passing.at[u, i], pass_send, pass_recv.at[u, i], here, peers[u + 1])
            elif s:
                u = s - 1
                push(both.at[i, :, half_cols(peers[s], u)], piece_half(s, i, u), half_send, half_recv.at[u, i], here, peers[s])

    def pass_on(i):
        for u in range(2):
            turn = 2 - u
            arrived(passing.at[u, i], pass_recv.at[u, i])
            passed[u, i] = (passing[u, i].astype(F32) + both[i, :, half_cols(peers[turn], u)].astype(F32)).astype(BF16)
            push(passed.at[u, i], piece_half(turn, i, u), sum_send, sum_recv.at[turn - 1, i], here, peers[turn])

    def reduce_tp(i):
        for s in (1, 2):
            arrived(piece_half(s, i, s - 1), half_recv.at[s - 1, i])
            arrived(piece_half(s, i, 2 - s), sum_recv.at[s - 1, i])
        acc = both[i, :, cols(t)].astype(F32) + pieces[0, i].astype(F32) + pieces[1, i].astype(F32)
        if i == 0:
            back_rows[z] = acc.astype(BF16)
        else:
            total[i] = acc.astype(BF16)
            push(total.at[i], back_rows.at[z], home_send, home_recv.at[z], order[i] * 2 + c, t)

    g_tile = min(512, width)

    def input_tiles(begin, end):
        @pl.loop(begin, end)
        def _(j):
            at = pl.ds(pl.multiple_of(j * g_tile, g_tile), g_tile)
            columns = x_all[:, :, :, at].reshape(zs * rows, g_tile).T
            for i, (grad, full) in enumerate(((gate_grad, gate_full), (up_grad, up_full))):
                term = jnp.dot(columns, grad[...].reshape(zs * rows, hid), preferred_element_type=F32)
                full[at, :] = term.astype(BF16)
                norms[pl.ds(i, 1), at] = lane_sums(term * term)

        if end == n_in:
            store(4, gate_full, gate_out)
            store(5, up_full, up_out)

    def down_tiles():
        turned = hidden[...].reshape(zs * rows, hid).T
        folded[...] = jnp.zeros_like(folded)

        @pl.loop(0, width // g_tile)
        def _(j):
            at = pl.ds(pl.multiple_of(j * g_tile, g_tile), g_tile)
            term = jnp.dot(turned, y_all[:, :, :, at].reshape(zs * rows, g_tile), preferred_element_type=F32)
            down_full[:, at] = term.astype(BF16)
            term = term * term
            acc = term[:, :128]
            for k in range(1, g_tile // 128):
                acc = acc + term[:, k * 128:(k + 1) * 128]
            folded[...] += acc

        store(6, down_full, down_out)
        out_down_norms[...] = jnp.sum(folded[...].T, axis=0, keepdims=True)
        store(3, out_down_norms, down_norms_out)

    def send_norms():
        for s in range(1, n_tp):
            push(norms, norm_pieces.at[s], tn_send, tn_recv.at[s], here, peers[s])

    def swap_scores():
        push(scores.at[1 - c], other_scores, cs_send, cs_recv, mate, t)

    def spread_scores():
        arrived(other_scores, cs_recv)
        both_scores[...] = scores[c] + other_scores[...]
        for s in range(1, n_tp):
            push(both_scores, score_pieces.at[s], ts_send, ts_recv.at[s], here, peers[s])

    def home_scores():
        acc = both_scores[...]
        for s in range(1, n_tp):
            arrived(score_pieces.at[s], ts_recv.at[s])
            acc = acc + score_pieces[s]
        total_scores[...] = acc
        for i in range(1, zs):
            push(total_scores.at[i], back_scores.at[z], es_send, es_recv.at[z], order[i] * 2 + c, t)
        back_scores[z] = total_scores[0]

    def close_norms():
        acc = norms[...]
        for s in range(1, n_tp):
            arrived(norm_pieces.at[s], tn_recv.at[s])
            acc = acc + norm_pieces[s]
        out_norms[...] = acc
        store(2, out_norms, norms_out)

    def close_scores():
        for q in order[1:]:
            arrived(back_scores.at[q], es_recv.at[q])
        for k in range(len(picks)):
            found = jnp.zeros((1, tok), F32)
            for e in range(zs):
                column = jnp.broadcast_to(back_scores[e], (8, back_scores.shape[2])).T[:cap, :1]
                found = found + jnp.sum(jnp.where(matches(e)[k], column, 0.0), axis=0, keepdims=True)
            out_mixing[k:k + 1, :] = found / mixing[k:k + 1, :]
        store(1, out_mixing, mixing_out)

    def close_tokens():
        for q in order[1:]:
            arrived(back_rows.at[q], home_recv.at[q])
        acc = jnp.zeros((tok, part), F32)
        for e in range(zs):
            pick = sum(hit.astype(F32) for hit in matches(e)).astype(BF16)
            acc = acc + lax.dot_general(pick, back_rows[e], first, preferred_element_type=F32)
        out_tokens[...] = acc.astype(BF16)
        store(0, out_tokens, tokens_out)

    n_in = width // g_tile
    cross(1)

    @pl.when(outer == 0)
    def _():
        cross(3)
        cross(2)

    spread(0)
    turn_down()
    relay(0)
    turn_in(0)
    spread(1)
    turn_in(1)
    finish(0)

    @pl.when(outer == 1)
    def _():
        cross(2)
        cross(3)

    relay(1)
    forward(0)
    spread(2)
    row_terms(0)
    finish(1)
    forward(1)
    relay(2)
    spread(3)
    row_terms(1)
    finish(2)
    relay(3)
    reduce_core(0)
    reduce_core(1)
    forward(2)
    row_terms(2)
    finish(3)
    pass_on(0)
    forward(3)
    swap_scores()
    pass_on(1)
    reduce_core(2)
    row_terms(3)
    spread_scores()
    pass_on(2)
    reduce_core(3)
    reduce_tp(0)
    reduce_tp(1)
    input_tiles(0, n_in // 2)
    pass_on(3)
    home_scores()
    reduce_tp(2)
    input_tiles(n_in // 2, n_in)
    send_norms()
    reduce_tp(3)
    down_tiles()
    close_norms()
    close_scores()
    close_tokens()
    for copy in stores:
        copy.wait()
    for a in range(2):
        arrived(puts[a].at[pl.ds(0, zs - 1)], ep_send.at[a])
        arrived(alls[a].at[:, 0], core_send.at[a])
        arrived(alls[a].at[:, 0, :, pl.ds(0, 2 * part)], tp_send.at[a])
        arrived(alls[a].at[:, 0, :, pl.ds(0, part)], fwd_send.at[a])
    arrived(other, swap_send)
    for sem in (pass_send, half_send, sum_send):
        arrived(passing, sem)
    arrived(total.at[pl.ds(0, zs - 1)], home_send)
    arrived(other_scores, cs_send)
    arrived(score_pieces.at[pl.ds(0, n_tp - 1)], ts_send)
    arrived(norm_pieces.at[pl.ds(0, n_tp - 1)], tn_send)
    arrived(total_scores.at[pl.ds(0, zs - 1)], es_send)


def settle_kernel(*refs):
    count = len(refs) // 2
    sem = refs[-1]
    copies = [pltpu.make_async_copy(refs[i], refs[count + i], sem.at[i]) for i in range(count)]
    for copy in copies:
        copy.start()
    for copy in copies:
        copy.wait()


def settle(arrays):
    far = pl.BlockSpec(memory_space=pltpu.HBM)
    vm = pl.BlockSpec(memory_space=pltpu.VMEM)
    return pl.pallas_call(
        settle_kernel,
        out_shape=tuple(jax.ShapeDtypeStruct(a.shape, a.dtype) for a in arrays),
        in_specs=[vm] * len(arrays),
        out_specs=(far,) * len(arrays),
        scratch_shapes=[pltpu.SemaphoreType.DMA((len(arrays),))],
        compiler_params=pltpu.CompilerParams(vmem_limit_bytes=2 << 20),
        name="settle",
    )(*[pltpu.with_memory_space_constraint(a, pltpu.VMEM) for a in arrays])


def fused(routing, mixing, tokens, upstream, w_gate, w_up, w_down, zs, n_tp, cap):
    top, tok = routing.shape
    part = tokens.shape[1]
    width, hid = w_gate.shape
    anywhere = pl.BlockSpec(memory_space=pl.ANY)
    far = pl.BlockSpec(memory_space=pltpu.HBM)
    dma = pltpu.SemaphoreType.DMA
    line = -(-cap // 128) * 128

    def room(*shape, kind=BF16):
        return pltpu.VMEM(shape, kind)

    return pl.pallas_call(
        functools.partial(fused_kernel, zs, n_tp, part, cap, tok),
        out_shape=(
            room(tok, part), room(top, tok, kind=F32), room(2, width, kind=F32), room(1, hid, kind=F32),
            room(width, hid), room(width, hid), room(hid, width),
        ),
        in_specs=[far] * 7,
        out_specs=(anywhere,) * 7,
        scratch_shapes=[
            room(tok, part), room(top, tok, kind=F32), room(2, width, kind=F32), room(1, hid, kind=F32),
            room(width, hid), room(width, hid), room(hid, width),
            room(top, tok, kind=jnp.int32), room(top, tok, kind=F32), room(tok, part), room(tok, part),
            room(width, hid), room(width, hid), room(hid, width), room(hid, width), room(hid, width), room(width, hid),
            room(zs, cap, part), room(zs, cap, part), room(zs, 2, cap, width), room(zs, 2, cap, width),
            room(zs, 2, cap, hid), room(zs, 2, cap, hid), room(zs, 2, cap, hid), room(top, tok, kind=jnp.int32),
            room(zs, 2, cap, width), room(zs, cap, width), room(zs, cap, width),
            room(2, zs, cap, part // 2), room(2, zs, cap, part // 2), room(2, zs, cap, part),
            room(zs, cap, part), room(zs, cap, part),
            room(2, zs, 1, line, kind=F32), room(zs, 1, line, kind=F32), room(zs, 1, line, kind=F32),
            room(n_tp, zs, 1, line, kind=F32), room(zs, 1, line, kind=F32), room(zs, 1, line, kind=F32),
            room(2, width, kind=F32), room(n_tp, 2, width, kind=F32), room(hid, 128, kind=F32),
            dma((7,)), dma((7,)), dma((2,)), dma((2,)), dma((2, zs)), dma((2,)), dma((2, zs, n_tp)),
            dma((2,)), dma((2,)), dma((2, zs, n_tp)),
            dma, dma((zs, n_tp)), dma, dma((2, zs)), dma, dma((2, zs)), dma, dma((2, zs)),
            dma, dma, dma, dma((n_tp,)), dma, dma((n_tp,)), dma, dma((zs,)), dma, dma((zs,)),
        ],
        compiler_params=pltpu.CompilerParams(collective_id=2, has_side_effects=True, vmem_limit_bytes=50 << 20),
        name="fused",
    )(*[pltpu.with_memory_space_constraint(a, pltpu.HBM) for a in (routing, mixing, tokens, upstream, w_gate, w_up, w_down)])


def on_device(tokens, routing, mixing, gate_matrix, up_matrix, down_matrix, upstream):
    experts = lax.axis_size("ep") // 2
    n_tp = lax.axis_size("tp")
    tok_rows, part = tokens.shape
    top = routing.shape[1]
    capacity = 5 * top * tok_rows // (4 * experts)
    if experts == 4 and n_tp == 4 and capacity % 16 == 0 and capacity <= 128:
        results = fused(
            routing.T, mixing.T, tokens, upstream, gate_matrix[0], up_matrix[0], down_matrix[0],
            experts, n_tp, capacity,
        )
        grads, mixing_grad, norms_all, down_norms, gate_full, up_full, down_full = settle(results)
        return (
            grads, mixing_grad.T, gate_full[None], up_full[None], down_full[None], norms_all[None], down_norms,
        )
    slots = experts * capacity
    flat = routing.reshape(-1)
    choose = (flat[:, None] == jnp.arange(experts, dtype=jnp.int32)[None, :]).astype(BF16)
    pairs = top * tok_rows
    before = (jnp.arange(pairs)[:, None] > jnp.arange(pairs)[None, :]).astype(BF16)
    earlier = jnp.dot(before, choose, preferred_element_type=F32)
    target = flat * capacity + jnp.sum(earlier * choose.astype(F32), axis=1).astype(jnp.int32)
    spot = target.reshape(tok_rows, top)
    matches = (spot[:, :, None] == jnp.arange(slots, dtype=jnp.int32)[None, None, :])
    by_token = jnp.any(matches, axis=1).astype(BF16)
    scaled = (mixing[:, :, None] * upstream[:, None, :].astype(F32)).astype(BF16)
    rows_first = (((0,), (0,)), ((), ()))
    placed_x = lax.dot_general(by_token, tokens, rows_first, preferred_element_type=F32).astype(BF16)
    placed_y = lax.dot_general(
        matches.reshape(pairs, slots).astype(BF16), scaled.reshape(pairs, part), rows_first,
        preferred_element_type=F32,
    ).astype(BF16)
    x_all, y_all = dispatch(
        placed_x.reshape(experts, capacity, part), placed_y.reshape(experts, capacity, part), experts, n_tp
    )
    width = n_tp * part
    row_count = 2 * slots
    x = x_all.reshape(row_count, width)
    y = y_all.reshape(row_count, width)
    w_gate, w_up, w_down = gate_matrix[0], up_matrix[0], down_matrix[0]
    cols = (((1,), (1,)), ((), ()))
    gate_pre = jnp.dot(x, w_gate, preferred_element_type=F32)
    up_pre = jnp.dot(x, w_up, preferred_element_type=F32)
    back = lax.dot_general(y, w_down, cols, preferred_element_type=F32)
    sig = jax.nn.sigmoid(gate_pre)
    act = gate_pre * sig
    hidden = act * up_pre
    gate_grad = (back * up_pre * sig * (1.0 + gate_pre * (1.0 - sig))).astype(BF16)
    up_grad = (back * act).astype(BF16)
    scores = jnp.sum(hidden * back, axis=1)
    line = -(-capacity // 128) * 128
    scores = jnp.pad(scores.reshape(2, experts, 1, capacity), ((0, 0), (0, 0), (0, 0), (0, line - capacity)))
    back_rows, back_scores, norms_all, down_norms, gate_full, up_full, down_full = send_back(
        gate_grad, up_grad, w_gate, w_up, x, hidden.astype(BF16), y, scores, experts, n_tp
    )
    token_gradient = jnp.dot(
        by_token, back_rows.reshape(slots, part), preferred_element_type=F32
    ).astype(BF16)
    pair_scores = back_scores[:, 0, :capacity].reshape(slots)
    mixing_gradient = jnp.sum(jnp.where(matches, pair_scores[None, None, :], 0.0), axis=2) / mixing
    return (
        token_gradient,
        mixing_gradient,
        gate_full[None],
        up_full[None],
        down_full[None],
        norms_all[None],
        down_norms,
    )


def solution(mesh):
    placed = (
        P("ep", "tp"), P("ep", None), P("ep", None), P("ep", None, "tp"),
        P("ep", None, "tp"), P("ep", "tp", None), P("ep", "tp"),
    )
    return jax.shard_map(
        on_device,
        mesh=mesh,
        in_specs=placed,
        out_specs=(
            P("ep", "tp"), P("ep", None), P("ep", None, "tp"), P("ep", None, "tp"),
            P("ep", "tp", None), P("ep", None, None), P("ep", "tp"),
        ),
        check_vma=False,
    )
```

```python
import functools

import jax
import jax.numpy as jnp
from jax import lax
from jax.experimental import pallas as pl
from jax.experimental.pallas import tpu as pltpu
from jax.sharding import PartitionSpec as P

MESH = pl.DeviceIdType.MESH
F32 = jnp.float32
BF16 = jnp.bfloat16


def send(src, dst, send_sem, recv_sem, ep, tp):
    copy = pltpu.make_async_remote_copy(
        src_ref=src, dst_ref=dst, send_sem=send_sem, recv_sem=recv_sem,
        device_id=(ep, tp), device_id_type=MESH,
    )
    copy.start()
    return copy


def arrived(ref, sem):
    pltpu.make_async_copy(ref, ref, sem).wait()


def places():
    ep, tp = lax.axis_index("ep"), lax.axis_index("tp")
    return ep // 2, ep % 2, tp


def tp_peer(tp, step, n_tp):
    if n_tp == 4:
        x, y = tp % 2, tp // 2
        return ((1 - y) if step // 2 else y) * 2 + ((1 - x) if step % 2 else x)
    return (tp + step) % n_tp


def tp_from(tp, step, n_tp):
    if n_tp == 4:
        return tp_peer(tp, step, n_tp)
    return (tp + n_tp - step) % n_tp


def greet(zs, n_tp, z, c, t):
    barrier = pltpu.get_barrier_semaphore()
    for k in range(1, zs):
        pl.semaphore_signal(barrier, inc=1, device_id=((z + k) % zs * 2 + c, t), device_id_type=MESH)
    for k in range(1, n_tp):
        pl.semaphore_signal(barrier, inc=1, device_id=(z * 2 + c, (t + k) % n_tp), device_id_type=MESH)
    pl.semaphore_signal(barrier, inc=1, device_id=(z * 2 + 1 - c, t), device_id_type=MESH)
    pl.semaphore_wait(barrier, zs + n_tp - 1)


def distances(zs):
    order = []
    for k in range(1, zs // 2 + 1):
        order.append(k)
        if zs - k != k:
            order.append(zs - k)
    return order


def dispatch_kernel(
    zs, n_tp, part, x_in, y_in, x_out, y_out, ep_send, ep_recv, tp_send, tp_recv,
    fwd_send, core_send, core_recv,
):
    z, c, t = places()
    chunks = zs if zs <= 4 else 1
    span = zs // chunks
    ins, outs = (x_in, y_in), (x_out, y_out)
    greet(zs, n_tp, z, c, t)

    def block(a, core, q, feat):
        cols = pl.ds(pl.multiple_of(feat * part, part), part)
        return outs[a].at[core, pl.ds(q * span, span), :, cols]

    def mine(a):
        cols = pl.ds(pl.multiple_of(t * part, part), part)
        return outs[a].at[c, z, :, cols]

    sent = []
    home = z // span
    for a in range(2):
        pltpu.make_async_copy(ins[a].at[z], mine(a), ep_recv.at[a, home]).start()
    for k in distances(zs):
        for a in range(2):
            dest = (z + k) % zs
            sent.append(send(ins[a].at[dest], mine(a), ep_send.at[a, k], ep_recv.at[a, home], dest * 2 + c, t))

    direct = (1, 2) if n_tp == 4 else range(1, n_tp)

    def to_core(a, q, feat):
        ref = block(a, c, q, feat)
        sent.append(send(ref, ref, core_send.at[a, q, feat], core_recv.at[a, q, feat], z * 2 + 1 - c, t))

    def spread(q):
        for a in range(2):
            ref = block(a, c, q, t)
            arrived(ref, ep_recv.at[a, q])
            for s in direct:
                sent.append(send(ref, ref, tp_send.at[a, q, s], tp_recv.at[a, q, t], z * 2 + c, tp_peer(t, s, n_tp)))
            to_core(a, q, t)

    def relay(q):
        if n_tp == 4:
            for a, s in ((0, 1), (1, 2), (1, 1), (0, 2)):
                feat = tp_from(t, s, n_tp)
                ref = block(a, c, q, feat)
                arrived(ref, tp_recv.at[a, q, feat])
                if s == a + 1:
                    sent.append(send(ref, ref, fwd_send.at[a, q], tp_recv.at[a, q, feat], z * 2 + c, tp_peer(t, 3 - s, n_tp)))
                to_core(a, q, feat)
        else:
            for s in direct:
                feat = tp_from(t, s, n_tp)
                for a in range(2):
                    arrived(block(a, c, q, feat), tp_recv.at[a, q, feat])
                    to_core(a, q, feat)

    def finish(q):
        if n_tp == 4:
            feat = tp_from(t, 3, n_tp)
            for a in range(2):
                arrived(block(a, c, q, feat), tp_recv.at[a, q, feat])
                to_core(a, q, feat)

    if chunks == 1:
        order = [0]
    else:
        order = [z] + [(z + zs - k) % zs for k in distances(zs)]
    for i in range(chunks + 2):
        if i < chunks:
            spread(order[i])
        if 1 <= i <= chunks:
            relay(order[i - 1])
        if i >= 2:
            finish(order[i - 2])
    for a in range(2):
        for q in range(chunks):
            for feat in range(n_tp):
                arrived(block(a, 1 - c, q, feat), core_recv.at[a, q, feat])
    for copy in sent:
        copy.wait_send()


def dispatch(x, y, zs, n_tp):
    _, cap, part = x.shape
    chunks = zs if zs <= 4 else 1
    out = jax.ShapeDtypeStruct((2, zs, cap, n_tp * part), BF16)
    vm = pl.BlockSpec(memory_space=pltpu.VMEM)
    dma = pltpu.SemaphoreType.DMA
    return pl.pallas_call(
        functools.partial(dispatch_kernel, zs, n_tp, part),
        out_shape=(out, out),
        in_specs=[vm, vm],
        out_specs=(vm, vm),
        scratch_shapes=[
            dma((2, zs)), dma((2, chunks)), dma((2, chunks, n_tp)), dma((2, chunks, n_tp)),
            dma((2, chunks)), dma((2, chunks, n_tp)), dma((2, chunks, n_tp)),
        ],
        compiler_params=pltpu.CompilerParams(collective_id=0, has_side_effects=True, vmem_limit_bytes=48 << 20),
        name="dispatch",
    )(x, y)


def hail(zs, n_tp, z, c, t):
    barrier = pltpu.get_barrier_semaphore()
    for k in range(1, zs):
        pl.semaphore_signal(barrier, inc=1, device_id=((z + k) % zs * 2 + c, t), device_id_type=MESH)
    for k in range(1, n_tp):
        pl.semaphore_signal(barrier, inc=1, device_id=(z * 2 + c, (t + k) % n_tp), device_id_type=MESH)
    pl.semaphore_signal(barrier, inc=1, device_id=(z * 2 + 1 - c, t), device_id_type=MESH)
    return lambda: pl.semaphore_wait(barrier, zs + n_tp - 1)


def lane_sums(square):
    folded = square[:, :128]
    for k in range(1, square.shape[1] // 128):
        folded = folded + square[:, k * 128:(k + 1) * 128]
    return jnp.sum(folded.T, axis=0, keepdims=True)


def return_kernel(
    zs, n_tp, part,
    gate_hbm, up_hbm, w_gate_hbm, w_up_hbm, x_hbm, hidden_hbm, y_hbm, scores,
    out_rows, out_scores, out_norms, out_down_norms, gate_out, up_out, down_out,
    gate_grad, up_grad, w_gate, w_up, x, hidden, y, gate_full, up_full, down_full, norms, folded,
    all_rows, other, other_scores, both, both_scores, pieces, score_pieces, norm_pieces, total, total_scores,
    passing, passed, pass_send, pass_recv, sum_send, sum_recv, load_sem, store_sem,
    core_send, core_recv, cs_send, cs_recv, tp_send, tp_recv, ts_send, ts_recv,
    tn_send, tn_recv, ep_send, ep_recv, es_send, es_recv,
):
    z, c, t = places()
    chunks = zs if zs <= 4 else 1
    span = zs // chunks
    cap = out_rows.shape[1]
    width, hid = w_gate.shape
    half = zs * cap
    everyone_in = hail(zs, n_tp, z, c, t)
    loads = []
    for i, (src, dst) in enumerate((
        (gate_hbm, gate_grad), (up_hbm, up_grad), (w_gate_hbm, w_gate), (w_up_hbm, w_up),
        (x_hbm, x), (hidden_hbm, hidden), (y_hbm, y),
    )):
        copy = pltpu.make_async_copy(src, dst, load_sem.at[i])
        copy.start()
        loads.append(copy)
    stores = []

    def store(i, src, dst):
        copy = pltpu.make_async_copy(src, dst, store_sem.at[i])
        copy.start()
        stores.append(copy)

    across = (((1,), (1,)), ((), ()))
    down = (((0,), (0,)), ((), ()))
    tile = min(256, width)

    def row_terms():
        @pl.loop(0, width // tile)
        def _(j):
            at = pl.ds(pl.multiple_of(j * tile, tile), tile)
            term = (
                lax.dot_general(gate_grad[...].reshape(2 * half, hid), w_gate[at, :], across, preferred_element_type=F32)
                + lax.dot_general(up_grad[...].reshape(2 * half, hid), w_up[at, :], across, preferred_element_type=F32)
            ).astype(BF16)
            all_rows[0, :, at] = term[:half]
            all_rows[1, :, at] = term[half:]

    sent = []
    if chunks == 1:
        order = [0]
    else:
        order = [(z + k) % zs for k in reversed(distances(zs))] + [z]
    mate = z * 2 + 1 - c

    def rows_of(q):
        if chunks == 1:
            return slice(None)
        return pl.ds(pl.multiple_of(q * cap, cap), cap)

    for copy in loads[:4]:
        copy.wait()
    row_terms()
    everyone_in()
    for q in order:
        sent.append(send(all_rows.at[1 - c, rows_of(q)], other.at[rows_of(q)], core_send.at[q], core_recv.at[q], mate, t))
    sent.append(send(scores.at[1 - c], other_scores, cs_send, cs_recv, mate, t))

    def cols(feat):
        return pl.ds(pl.multiple_of(feat * part, part), part)

    def reduce_core(q):
        at = rows_of(q)
        arrived(other.at[at], core_recv.at[q])
        both[at, :] = (all_rows[c, at, :].astype(F32) + other[at, :].astype(F32)).astype(BF16)
        if n_tp == 4:
            far_side = tp_peer(t, 3, n_tp)
            for s in (1, 2):
                sent.append(send(both.at[at, half_cols(far_side, s - 1)], passing.at[s - 1, at], pass_send.at[s - 1, q], pass_recv.at[s - 1, q], z * 2 + c, tp_peer(t, s, n_tp)))
            for s in (1, 2):
                feat = tp_peer(t, s, n_tp)
                sent.append(send(both.at[at, half_cols(feat, s - 1)], piece_half(s, at, s - 1), tp_send.at[s, q], tp_recv.at[s, q], z * 2 + c, feat))
        else:
            for s in reversed(range(1, n_tp)):
                feat = tp_peer(t, s, n_tp)
                sent.append(send(both.at[at, cols(feat)], pieces.at[s, at], tp_send.at[s, q], tp_recv.at[s, q], z * 2 + c, feat))

    def half_cols(feat, u):
        return pl.ds(pl.multiple_of(feat * part + u * (part // 2), part // 2), part // 2)

    def piece_half(s, at, u):
        return pieces.at[s, at, pl.ds(u * (part // 2), part // 2)]

    def pass_on(q):
        if n_tp == 4:
            at = rows_of(q)
            for s in (1, 2):
                u, turn = s - 1, 3 - s
                feat = tp_peer(t, turn, n_tp)
                arrived(passing.at[u, at], pass_recv.at[u, q])
                passed[u, at, :] = (passing[u, at, :].astype(F32) + both[at, half_cols(feat, u)].astype(F32)).astype(BF16)
                sent.append(send(passed.at[u, at], piece_half(turn, at, u), sum_send.at[turn, q], sum_recv.at[turn, q], z * 2 + c, feat))

    for q in order:
        reduce_core(q)
    arrived(other_scores, cs_recv)
    both_scores[...] = scores[c] + other_scores[...]
    for s in range(1, n_tp):
        sent.append(send(both_scores, score_pieces.at[s], ts_send.at[s], ts_recv.at[s], z * 2 + c, tp_peer(t, s, n_tp)))

    def reduce_tp(q):
        at = rows_of(q)
        if n_tp == 4:
            for s in (1, 2):
                arrived(piece_half(s, at, s - 1), tp_recv.at[s, q])
                arrived(piece_half(s, at, 2 - s), sum_recv.at[s, q])
        else:
            for s in reversed(range(1, n_tp)):
                arrived(pieces.at[s, at], tp_recv.at[s, q])
        for j in range(span):
            sub = at if chunks > 1 else slice(j * cap, (j + 1) * cap)
            acc = both[sub, cols(t)].astype(F32)
            for s in (1, 2) if n_tp == 4 else range(1, n_tp):
                acc = acc + pieces[s, sub, :].astype(F32)
            total[q * span + j] = acc.astype(BF16)

    def go_home(dest, k):
        sent.append(send(total.at[dest], out_rows.at[z], ep_send.at[k], ep_recv.at[k], dest * 2 + c, t))

    def input_tiles(first, last):
        @pl.loop(first * tile // g_tile, last * tile // g_tile)
        def _(j):
            at = pl.ds(pl.multiple_of(j * g_tile, g_tile), g_tile)
            columns = x[:, at].T
            for i, (grad, full) in enumerate(((gate_grad, gate_full), (up_grad, up_full))):
                term = jnp.dot(columns, grad[...].reshape(2 * half, hid), preferred_element_type=F32)
                full[at, :] = term.astype(BF16)
                norms[pl.ds(i, 1), at] = lane_sums(term * term)

    h_tile = min(256, hid)
    g_tile = min(512, width)
    wide = min(512, width)

    def down_tiles(i):
        at = slice(i * h_tile, (i + 1) * h_tile)
        folded[...] = jnp.zeros_like(folded)
        turned = hidden[:, at].T

        @pl.loop(0, width // wide)
        def _(j):
            lanes = pl.ds(pl.multiple_of(j * wide, wide), wide)
            term = jnp.dot(turned, y[:, lanes], preferred_element_type=F32)
            down_full[at, lanes] = term.astype(BF16)
            square = term * term
            acc = square[:, :128]
            for k in range(1, wide // 128):
                acc = acc + square[:, k * 128:(k + 1) * 128]
            folded[...] += acc

        out_down_norms[:, at] = jnp.sum(folded[...].T, axis=0, keepdims=True)

    away = list(reversed(distances(zs)))
    n_tiles = width // tile

    def phase_input(first, last):
        if first == 0:
            loads[4].wait()
        input_tiles(first, last)
        if last == n_tiles:
            store(0, gate_full, gate_out)
            store(1, up_full, up_out)
            for s in range(1, n_tp):
                sent.append(send(norms, norm_pieces.at[s], tn_send.at[s], tn_recv.at[s], z * 2 + c, tp_peer(t, s, n_tp)))

    def phase_down(first, last):
        if first == 0:
            loads[5].wait()
            loads[6].wait()
        for i in range(first, last):
            down_tiles(i)
        if last == hid // h_tile:
            store(2, down_full, down_out)

    h_count = hid // h_tile
    phases = [
        lambda: phase_input(0, n_tiles // 2),
        lambda: phase_input(n_tiles // 2, n_tiles),
        lambda: phase_down(0, h_count // 2) if h_count > 1 else None,
        lambda: phase_down(h_count // 2, h_count),
    ]
    if chunks < len(phases):
        for phase in phases:
            phase()
        phases = []
    pass_on(order[0])
    if chunks > 1:
        pass_on(order[1])
    for i in range(chunks):
        if i < len(phases):
            phases[i]()
        if i + 2 < chunks:
            pass_on(order[i + 2])
        reduce_tp(order[i])
        if chunks > 1:
            if i < len(away):
                go_home(order[i], away[i])
        else:
            for k in away:
                go_home((z + k) % zs, k)
        if i == 0:
            for s in range(1, n_tp):
                arrived(score_pieces.at[s], ts_recv.at[s])
            acc = both_scores[...]
            for s in range(1, n_tp):
                acc = acc + score_pieces[s]
            total_scores[...] = acc
            for k in away:
                dest = (z + k) % zs
                sent.append(send(total_scores.at[dest], out_scores.at[z], es_send.at[k], es_recv.at[k], dest * 2 + c, t))
            out_scores[z] = total_scores[z]
    out_rows[z] = total[z]
    acc = norms[...]
    for s in range(1, n_tp):
        arrived(norm_pieces.at[s], tn_recv.at[s])
        acc = acc + norm_pieces[s]
    out_norms[...] = acc
    for k in away:
        src = (z + zs - k) % zs
        arrived(out_scores.at[src], es_recv.at[k])
        arrived(out_rows.at[src], ep_recv.at[k])
    for copy in stores:
        copy.wait()
    for copy in sent:
        copy.wait_send()


def send_back(gate_grad, up_grad, w_gate, w_up, x, hidden, y, scores, zs, n_tp):
    rows, width = x.shape
    hid = hidden.shape[1]
    part, half = width // n_tp, rows // 2
    cap = half // zs
    chunks = zs if zs <= 4 else 1
    vm = pl.BlockSpec(memory_space=pltpu.VMEM)
    far = pl.BlockSpec(memory_space=pltpu.HBM)
    dma = pltpu.SemaphoreType.DMA
    line = scores.shape[2:]
    gradient = jax.ShapeDtypeStruct((width, hid), BF16)
    return pl.pallas_call(
        functools.partial(return_kernel, zs, n_tp, part),
        out_shape=(
            jax.ShapeDtypeStruct((zs, cap, part), BF16),
            jax.ShapeDtypeStruct((zs,) + line, F32),
            jax.ShapeDtypeStruct((2, width), F32),
            jax.ShapeDtypeStruct((1, hid), F32),
            gradient, gradient, jax.ShapeDtypeStruct((hid, width), BF16),
        ),
        in_specs=[far] * 7 + [vm],
        out_specs=(vm,) * 4 + (far,) * 3,
        scratch_shapes=[
            pltpu.VMEM((2, half, hid), BF16), pltpu.VMEM((2, half, hid), BF16),
            pltpu.VMEM((width, hid), BF16), pltpu.VMEM((width, hid), BF16),
            pltpu.VMEM((rows, width), BF16), pltpu.VMEM((rows, hid), BF16), pltpu.VMEM((rows, width), BF16),
            pltpu.VMEM((width, hid), BF16), pltpu.VMEM((width, hid), BF16), pltpu.VMEM((hid, width), BF16),
            pltpu.VMEM((2, width), F32), pltpu.VMEM((min(256, hid), 128), F32),
            pltpu.VMEM((2, half, width), BF16), pltpu.VMEM((half, width), BF16),
            pltpu.VMEM((zs,) + line, F32),
            pltpu.VMEM((half, width), BF16),
            pltpu.VMEM((zs,) + line, F32),
            pltpu.VMEM((n_tp, half, part), BF16),
            pltpu.VMEM((n_tp, zs) + line, F32),
            pltpu.VMEM((n_tp, 2, width), F32),
            pltpu.VMEM((zs, cap, part), BF16),
            pltpu.VMEM((zs,) + line, F32),
            pltpu.VMEM((2, half, part // 2), BF16), pltpu.VMEM((2, half, part // 2), BF16),
            dma((2, chunks)), dma((2, chunks)), dma((3, chunks)), dma((3, chunks)),
            dma((7,)), dma((3,)),
            dma((chunks,)), dma((chunks,)), dma, dma,
            dma((n_tp, chunks)), dma((n_tp, chunks)), dma((n_tp,)), dma((n_tp,)),
            dma((n_tp,)), dma((n_tp,)), dma((zs,)), dma((zs,)), dma((zs,)), dma((zs,)),
        ],
        compiler_params=pltpu.CompilerParams(collective_id=1, has_side_effects=True, vmem_limit_bytes=50 << 20),
        name="send_back",
    )(gate_grad.reshape(2, half, hid), up_grad.reshape(2, half, hid), w_gate, w_up, x, hidden, y, scores)


def fused_kernel(
    zs, n_tp, part, cap, tok,
    routing_hbm, mixing_hbm, tokens_hbm, upstream_hbm, w_gate_hbm, w_up_hbm, w_down_hbm,
    out_tokens, out_mixing, out_norms, out_down_norms, gate_full, up_full, down_full,
    routing, mixing, tokens, upstream, w_gate, w_up, w_down, gate_turned, up_turned, down_turned,
    x_put, y_put, x_all, y_all, gate_grad, up_grad, hidden, targets,
    all_rows, other, both, passing, passed, pieces, total, back_rows,
    scores, other_scores, both_scores, score_pieces, total_scores, back_scores,
    norms, norm_pieces,
    folded, hidden_turned, load_sem, own_sem, ep_send, ep_recv, tp_send, tp_recv, fwd_send, core_send, core_recv,
    swap_send, swap_recv, ring_send, pass_recv, sum_recv,
    cs_send, cs_recv, ts_send, ts_recv, tn_send, tn_recv, home_send, home_recv, es_send, es_recv,
):
    z, c, t = places()
    here, mate = z * 2 + c, z * 2 + 1 - c
    peers = [tp_peer(t, s, n_tp) for s in range(n_tp)]
    width, hid = w_gate.shape
    rows = 2 * cap
    loads = []
    for i, (src, dst) in enumerate((
        (routing_hbm, routing), (mixing_hbm, mixing), (tokens_hbm, tokens), (upstream_hbm, upstream),
        (w_down_hbm, w_down), (w_gate_hbm, w_gate), (w_up_hbm, w_up),
    )):
        copy = pltpu.make_async_copy(src, dst, load_sem.at[i])
        copy.start()
        loads.append(copy)
    everyone_in = hail(zs, n_tp, z, c, t)
    across = (((1,), (1,)), ((), ()))
    first = (((0,), (0,)), ((), ()))
    def push(src, dst, send_sem, recv_sem, ep, tp):
        send(src, dst, send_sem, recv_sem, ep, tp)

    def cols(feat):
        return pl.ds(pl.multiple_of(feat * part, part), part)

    def half_cols(feat, u):
        return pl.ds(pl.multiple_of(feat * part + u * (part // 2), part // 2), part // 2)

    lanes = -(-zs // 16) * 16
    experts_at = lax.broadcasted_iota(jnp.int32, (lanes, tok), 0)
    before = lax.broadcasted_iota(jnp.int32, (tok, tok), 0) < lax.broadcasted_iota(jnp.int32, (tok, tok), 1)
    for copy in loads[:2]:
        copy.wait()
    picks = [routing[k:k + 1, :] == experts_at for k in range(routing.shape[0])]
    chosen = sum(pick.astype(F32) for pick in picks)
    earlier = jnp.dot(chosen.astype(BF16), before.astype(F32).astype(BF16), preferred_element_type=F32)
    for k, pick in enumerate(picks):
        place = jnp.sum(jnp.where(pick, earlier, 0.0), axis=0, keepdims=True)
        targets[k:k + 1, :] = routing[k:k + 1, :] * cap + place.astype(jnp.int32)

    def matches(e):
        slots_at = lax.broadcasted_iota(jnp.int32, (cap, tok), 0) + e * cap
        return [targets[k:k + 1, :] == slots_at for k in range(len(picks))]

    for copy in loads[2:4]:
        copy.wait()
    for e in range(zs):
        hits = matches(e)
        pick = sum(hit.astype(F32) for hit in hits).astype(BF16)
        weight = sum(jnp.where(hit, mixing[k:k + 1, :], 0.0) for k, hit in enumerate(hits))
        x_put[e] = jnp.dot(pick, tokens[...], preferred_element_type=F32).astype(BF16)
        placed = jnp.dot(pick, upstream[...], preferred_element_type=F32)
        y_put[e] = (placed * jnp.sum(weight, axis=1, keepdims=True)).astype(BF16)
    scores[...] = jnp.zeros_like(scores)
    everyone_in()

    outer = (z - 1) * (z - 2) // 2
    order = [z, 1 + z % 2, 3 - 3 * (z // 2), (2 + 3 * z) % 5]
    lands = [0, 1 + 2 * outer, 3 - outer, 1 + outer]
    puts, alls = (x_put, y_put), (x_all, y_all)

    def block(a, i, core, feat):
        return alls[a].at[i, core, :, cols(feat)]

    def slab(a, i, feat, u):
        return alls[a].at[i, c, :, half_cols(feat, u)]

    for a in range(2):
        copy = pltpu.make_async_copy(puts[a].at[z], block(a, 0, c, t), own_sem)
        copy.start()

    def over(i):
        return [
            pltpu.make_async_remote_copy(
                src_ref=puts[a].at[order[i]], dst_ref=block(a, lands[i], c, t), send_sem=ep_send,
                recv_sem=ep_recv.at[a, lands[i]], device_id=(order[i] * 2 + c, t), device_id_type=MESH,
            )
            for a in range(2)
        ]

    def cross(i):
        for copy in over(i):
            copy.start()

    def to_core(a, i, feat, src=None):
        ref = block(a, i, c, feat)
        push(ref if src is None else src, ref, core_send, core_recv.at[i], mate, t)

    def spread(i, apart=False):
        halves = [pl.ds(u * (part // 2), part // 2) for u in range(2)]

        def land(a):
            if i:
                arrived(block(a, i, c, t), ep_recv.at[a, i])

        def near(a):
            for u in range(2):
                ref = slab(a, i, t, u)
                push(ref if i else puts[a].at[z, :, halves[u]], ref, tp_send, tp_recv.at[i, 2 * a + u], here, peers[1 + a])

        def other_way(a):
            ref = block(a, i, c, t)
            push(ref if i else puts[a].at[z], ref, tp_send, tp_recv.at[i, 4], here, peers[2 - a])

        def over_core(a):
            to_core(a, i, t, None if i else puts[a].at[z])

        if apart:
            for a in range(2):
                land(a)
                near(a)
                other_way(a)
                over_core(a)
        else:
            for step in (land, near, other_way, over_core):
                for a in range(2):
                    step(a)

    def relay(i):
        for u in range(2):
            for a in range(2):
                ref = slab(a, i, peers[1 + a], u)
                arrived(ref, tp_recv.at[i, 2 * a + u])
                push(ref, ref, fwd_send, tp_recv.at[i, 5], here, peers[2 - a])
        for a in range(2):
            to_core(a, i, peers[1 + a])

    def pair_of(i):
        return x_all.at[i, :, :, pl.ds(0, part)]

    def finish(i):
        arrived(pair_of(i), tp_recv.at[i, 4])
        for a in range(2):
            to_core(a, i, peers[2 - a])
        arrived(pair_of(i), tp_recv.at[i, 5])
        for a in range(2):
            to_core(a, i, peers[3])

    square = min(256, hid)
    eye = (
        lax.broadcasted_iota(jnp.int32, (square, square), 0) == lax.broadcasted_iota(jnp.int32, (square, square), 1)
    ).astype(F32).astype(BF16)

    def turn_down():
        loads[4].wait()

        @pl.loop(0, width // square, unroll=4)
        def _(j):
            at = pl.ds(pl.multiple_of(j * square, square), square)
            down_turned[at, :] = lax.dot_general(eye, w_down[:, at], across, preferred_element_type=F32).astype(BF16)

    def turn_in(a):
        loads[5 + a].wait()
        src, dst = ((w_gate, gate_turned), (w_up, up_turned))[a]

        @pl.loop(0, width // square, unroll=4)
        def _(j):
            at = pl.ds(pl.multiple_of(j * square, square), square)
            for h in range(hid // square):
                lines = slice(h * square, (h + 1) * square)
                dst[lines, at] = lax.dot_general(eye, src[at, lines], across, preferred_element_type=F32).astype(BF16)

    h_tile = min(256, hid)

    def forward(i):
        if i == 0:
            arrived(pair_of(0), own_sem)
        arrived(x_all.at[i], core_recv.at[i])
        for j in range(hid // h_tile):
            at = slice(j * h_tile, (j + 1) * h_tile)
            gate_pre = jnp.dot(x_all[i].reshape(rows, width), w_gate[:, at], preferred_element_type=F32)
            up_pre = jnp.dot(x_all[i].reshape(rows, width), w_up[:, at], preferred_element_type=F32)
            back = jnp.dot(y_all[i].reshape(rows, width), down_turned[:, at], preferred_element_type=F32)
            sig = jax.nn.sigmoid(gate_pre)
            act = gate_pre * sig
            low = act * up_pre
            gate_grad[i, :, :, at] = (back * up_pre * sig * (1.0 + gate_pre * (1.0 - sig))).astype(BF16).reshape(2, cap, h_tile)
            up_grad[i, :, :, at] = (back * act).astype(BF16).reshape(2, cap, h_tile)
            hidden[i, :, :, at] = low.astype(BF16).reshape(2, cap, h_tile)
            terms = low * back
            for core in range(2):
                scores[core, i, :, :cap] += lane_sums(terms[core * cap:(core + 1) * cap])

    def row_terms(i, steps=(3, 1, 2, 0)):
        for s in steps:
            at = cols(peers[s])
            term = (
                jnp.dot(gate_grad[i].reshape(rows, hid), gate_turned[:, at], preferred_element_type=F32)
                + jnp.dot(up_grad[i].reshape(rows, hid), up_turned[:, at], preferred_element_type=F32)
            ).astype(BF16)
            all_rows[i, :, :, at] = term.reshape(2, cap, part)
            push(all_rows.at[i, 1 - c, :, at], other.at[i, :, at], swap_send, swap_recv.at[i, 0 if s == 3 else 1], mate, t)

    def piece_half(s, i, u):
        return pieces.at[s - 1, i, :, pl.ds(u * (part // 2), part // 2)]

    def reduce_core(i):
        for s in (3, 1, 2, 0):
            at = cols(peers[s])
            if s == 3:
                arrived(other.at[i, :, at], swap_recv.at[i, 0])
            elif s == 1:
                arrived(other.at[i, :, pl.ds(0, (n_tp - 1) * part)], swap_recv.at[i, 1])
            both[i, :, at] = (all_rows[i, c, :, at].astype(F32) + other[i, :, at].astype(F32)).astype(BF16)
            if s == 3:
                for u in range(2):
                    push(both.at[i, :, half_cols(peers[3], u)], passing.at[u, i], ring_send, pass_recv.at[i], here, peers[u + 1])
            elif s:
                u = s - 1
                push(both.at[i, :, half_cols(peers[s], u)], piece_half(s, i, u), ring_send, sum_recv.at[i], here, peers[s])

    def pass_on(i):
        arrived(passing.at[:, i], pass_recv.at[i])
        for u in range(2):
            turn = 2 - u
            passed[u, i] = (passing[u, i].astype(F32) + both[i, :, half_cols(peers[turn], u)].astype(F32)).astype(BF16)
            push(passed.at[u, i], piece_half(turn, i, u), ring_send, sum_recv.at[i], here, peers[turn])

    def reduce_tp(i):
        arrived(pieces.at[:, i], sum_recv.at[i])
        acc = both[i, :, cols(t)].astype(F32) + pieces[0, i].astype(F32) + pieces[1, i].astype(F32)
        if i == 0:
            back_rows[z] = acc.astype(BF16)
        else:
            total[i] = acc.astype(BF16)
            push(total.at[i], back_rows.at[z], home_send, home_recv.at[z], order[i] * 2 + c, t)

    g_tile = min(512, width)

    def input_tiles(begin, end):
        @pl.loop(begin, end, unroll=min(2, end - begin))
        def _(j):
            at = pl.ds(pl.multiple_of(j * g_tile, g_tile), g_tile)
            columns = x_all[:, :, :, at].reshape(zs * rows, g_tile).T
            for i, (grad, full) in enumerate(((gate_grad, gate_full), (up_grad, up_full))):
                term = jnp.dot(columns, grad[...].reshape(zs * rows, hid), preferred_element_type=F32)
                full[at, :] = term.astype(BF16)
                norms[pl.ds(i, 1), at] = lane_sums(term * term)

    def turn_hidden():
        hidden_turned[...] = hidden[...].reshape(zs * rows, hid).T

    def down_tiles(begin, end):
        if begin == 0:
            folded[...] = jnp.zeros_like(folded)

        @pl.loop(begin, end, unroll=min(2, end - begin))
        def _(j):
            at = pl.ds(pl.multiple_of(j * g_tile, g_tile), g_tile)
            term = jnp.dot(hidden_turned[...], y_all[:, :, :, at].reshape(zs * rows, g_tile), preferred_element_type=F32)
            down_full[:, at] = term.astype(BF16)
            term = term * term
            acc = term[:, :128]
            for k in range(1, g_tile // 128):
                acc = acc + term[:, k * 128:(k + 1) * 128]
            folded[...] += acc

        if end == n_in:
            out_down_norms[...] = jnp.sum(folded[...].T, axis=0, keepdims=True)

    def send_norms():
        for s in range(1, n_tp):
            push(norms, norm_pieces.at[s], tn_send, tn_recv, here, peers[s])

    def swap_scores():
        push(scores.at[1 - c], other_scores, cs_send, cs_recv, mate, t)

    def spread_scores():
        arrived(other_scores, cs_recv)
        both_scores[...] = scores[c] + other_scores[...]
        for s in range(1, n_tp):
            push(both_scores, score_pieces.at[s], ts_send, ts_recv, here, peers[s])

    def home_scores():
        acc = both_scores[...]
        arrived(score_pieces.at[pl.ds(1, n_tp - 1)], ts_recv)
        for s in range(1, n_tp):
            acc = acc + score_pieces[s]
        total_scores[...] = acc
        for i in range(1, zs):
            push(total_scores.at[i], back_scores.at[z], es_send, es_recv, order[i] * 2 + c, t)
        back_scores[z] = total_scores[0]

    def close_norms():
        acc = norms[...]
        arrived(norm_pieces.at[pl.ds(1, n_tp - 1)], tn_recv)
        for s in range(1, n_tp):
            acc = acc + norm_pieces[s]
        out_norms[...] = acc

    def close_scores():
        arrived(back_scores.at[pl.ds(0, zs - 1)], es_recv)
        for k in range(len(picks)):
            found = jnp.zeros((1, tok), F32)
            for e in range(zs):
                column = jnp.broadcast_to(back_scores[e], (8, back_scores.shape[2])).T[:cap, :1]
                found = found + jnp.sum(jnp.where(matches(e)[k], column, 0.0), axis=0, keepdims=True)
            out_mixing[k:k + 1, :] = found / mixing[k:k + 1, :]

    def close_tokens():
        last = (2 * z + 1) % 5
        acc = jnp.zeros((tok, part), F32)
        for k in range(1, zs + 1):
            e = (last + k) % zs

            @pl.when(e != z)
            def _():
                arrived(back_rows.at[e], home_recv.at[e])

            pick = sum(hit.astype(F32) for hit in matches(e)).astype(BF16)
            acc = acc + lax.dot_general(pick, back_rows[e], first, preferred_element_type=F32)
        out_tokens[...] = acc.astype(BF16)

    n_in = width // g_tile
    cross(1)
    cross(3)

    @pl.when(outer == 1)
    def _():
        cross(2)

    spread(0)
    turn_down()
    relay(0)
    turn_in(0)
    spread(1)
    turn_in(1)
    finish(0)

    @pl.when(outer == 0)
    def _():
        cross(2)

    relay(1)
    forward(0)
    spread(2, True)
    row_terms(0)
    finish(1)
    forward(1)
    relay(2)
    spread(3)
    row_terms(1)
    finish(2)
    relay(3)
    reduce_core(1)
    forward(2)
    row_terms(2)
    finish(3)
    reduce_core(2)
    pass_on(1)
    forward(3)
    swap_scores()
    row_terms(3, (3, 1))
    pass_on(2)
    row_terms(3, (2, 0))
    spread_scores()
    turn_hidden()
    reduce_core(3)
    reduce_tp(1)
    reduce_core(0)
    input_tiles(0, n_in // 2)
    reduce_tp(2)
    home_scores()
    pass_on(3)
    input_tiles(n_in // 2, n_in)
    send_norms()
    pass_on(0)
    down_tiles(0, n_in // 2)
    reduce_tp(3)
    down_tiles(n_in // 2, n_in)
    reduce_tp(0)
    close_scores()
    close_norms()
    close_tokens()
    arrived(x_all.at[pl.ds(0, zs - 1), :, :, pl.ds(0, part)], ep_send)
    arrived(x_all, core_send)
    arrived(x_all.at[:, :, :, pl.ds(0, 2 * part)], tp_send)
    arrived(x_all.at[:, :, :, pl.ds(0, part)], fwd_send)
    arrived(other, swap_send)
    arrived(x_all.at[pl.ds(0, 3), :, :, pl.ds(0, zs * part // 2)], ring_send)
    arrived(total.at[pl.ds(0, zs - 1)], home_send)
    arrived(other_scores, cs_send)
    arrived(score_pieces.at[pl.ds(0, n_tp - 1)], ts_send)
    arrived(norm_pieces.at[pl.ds(0, n_tp - 1)], tn_send)
    arrived(total_scores.at[pl.ds(0, zs - 1)], es_send)


def settle_kernel(slices, *refs):
    count = len(refs) // 2
    sem = refs[-1]
    copies = []
    for i in range(count):
        lines = refs[i].shape[0]
        parts = slices if lines % (16 * slices) == 0 else 1
        for k in range(parts):
            at = pl.ds(k * (lines // parts), lines // parts)
            copies.append(pltpu.make_async_copy(refs[i].at[at], refs[count + i].at[at], sem.at[i, k]))
    for copy in copies:
        copy.start()
    for copy in copies:
        copy.wait()


def settle(arrays, slices=1):
    far = pl.BlockSpec(memory_space=pltpu.HBM)
    vm = pl.BlockSpec(memory_space=pltpu.VMEM)
    return pl.pallas_call(
        functools.partial(settle_kernel, slices),
        out_shape=tuple(jax.ShapeDtypeStruct(a.shape, a.dtype) for a in arrays),
        in_specs=[vm] * len(arrays),
        out_specs=(far,) * len(arrays),
        scratch_shapes=[pltpu.SemaphoreType.DMA((len(arrays), slices))],
        compiler_params=pltpu.CompilerParams(vmem_limit_bytes=2 << 20),
        name="settle",
    )(*[pltpu.with_memory_space_constraint(a, pltpu.VMEM) for a in arrays])


def fused(routing, mixing, tokens, upstream, w_gate, w_up, w_down, zs, n_tp, cap):
    top, tok = routing.shape
    part = tokens.shape[1]
    width, hid = w_gate.shape
    vm = pl.BlockSpec(memory_space=pltpu.VMEM)
    far = pl.BlockSpec(memory_space=pltpu.HBM)
    dma = pltpu.SemaphoreType.DMA
    line = -(-cap // 128) * 128

    def room(*shape, kind=BF16):
        return pltpu.VMEM(shape, kind)

    return pl.pallas_call(
        functools.partial(fused_kernel, zs, n_tp, part, cap, tok),
        out_shape=(
            room(tok, part), room(top, tok, kind=F32), room(2, width, kind=F32), room(1, hid, kind=F32),
            room(width, hid), room(width, hid), room(hid, width),
        ),
        in_specs=[far] * 7,
        out_specs=(vm,) * 7,
        scratch_shapes=[
            room(top, tok, kind=jnp.int32), room(top, tok, kind=F32), room(tok, part), room(tok, part),
            room(width, hid), room(width, hid), room(hid, width), room(hid, width), room(hid, width), room(width, hid),
            room(zs, cap, part), room(zs, cap, part), room(zs, 2, cap, width), room(zs, 2, cap, width),
            room(zs, 2, cap, hid), room(zs, 2, cap, hid), room(zs, 2, cap, hid), room(top, tok, kind=jnp.int32),
            room(zs, 2, cap, width), room(zs, cap, width), room(zs, cap, width),
            room(2, zs, cap, part // 2), room(2, zs, cap, part // 2), room(2, zs, cap, part),
            room(zs, cap, part), room(zs, cap, part),
            room(2, zs, 1, line, kind=F32), room(zs, 1, line, kind=F32), room(zs, 1, line, kind=F32),
            room(n_tp, zs, 1, line, kind=F32), room(zs, 1, line, kind=F32), room(zs, 1, line, kind=F32),
            room(2, width, kind=F32), room(n_tp, 2, width, kind=F32), room(hid, 128, kind=F32), room(hid, 2 * zs * cap),
            dma((7,)), dma, dma, dma((2, zs)), dma, dma((zs, 6)), dma, dma, dma((zs,)),
            dma, dma((zs, 2)), dma, dma((zs,)), dma((zs,)),
            dma, dma, dma, dma, dma, dma, dma, dma((zs,)), dma, dma,
        ],
        compiler_params=pltpu.CompilerParams(collective_id=2, has_side_effects=True, vmem_limit_bytes=50 << 20),
        name="fused",
    )(*[pltpu.with_memory_space_constraint(a, pltpu.HBM) for a in (routing, mixing, tokens, upstream, w_gate, w_up, w_down)])


def on_device(tokens, routing, mixing, gate_matrix, up_matrix, down_matrix, upstream):
    experts = lax.axis_size("ep") // 2
    n_tp = lax.axis_size("tp")
    tok_rows, part = tokens.shape
    top = routing.shape[1]
    capacity = 5 * top * tok_rows // (4 * experts)
    if experts == 4 and n_tp == 4 and capacity % 16 == 0 and capacity <= 128:
        results = fused(
            routing.T, mixing.T, tokens, upstream, gate_matrix[0], up_matrix[0], down_matrix[0],
            experts, n_tp, capacity,
        )
        grads, mixing_grad, norms_all, down_norms, gate_full, up_full, down_full = settle(results)
        return (
            grads, mixing_grad.T, gate_full[None], up_full[None], down_full[None], norms_all[None], down_norms,
        )
    slots = experts * capacity
    flat = routing.reshape(-1)
    choose = (flat[:, None] == jnp.arange(experts, dtype=jnp.int32)[None, :]).astype(BF16)
    pairs = top * tok_rows
    before = (jnp.arange(pairs)[:, None] > jnp.arange(pairs)[None, :]).astype(BF16)
    earlier = jnp.dot(before, choose, preferred_element_type=F32)
    target = flat * capacity + jnp.sum(earlier * choose.astype(F32), axis=1).astype(jnp.int32)
    spot = target.reshape(tok_rows, top)
    matches = (spot[:, :, None] == jnp.arange(slots, dtype=jnp.int32)[None, None, :])
    by_token = jnp.any(matches, axis=1).astype(BF16)
    scaled = (mixing[:, :, None] * upstream[:, None, :].astype(F32)).astype(BF16)
    rows_first = (((0,), (0,)), ((), ()))
    placed_x = lax.dot_general(by_token, tokens, rows_first, preferred_element_type=F32).astype(BF16)
    placed_y = lax.dot_general(
        matches.reshape(pairs, slots).astype(BF16), scaled.reshape(pairs, part), rows_first,
        preferred_element_type=F32,
    ).astype(BF16)
    x_all, y_all = dispatch(
        placed_x.reshape(experts, capacity, part), placed_y.reshape(experts, capacity, part), experts, n_tp
    )
    width = n_tp * part
    row_count = 2 * slots
    x = x_all.reshape(row_count, width)
    y = y_all.reshape(row_count, width)
    w_gate, w_up, w_down = gate_matrix[0], up_matrix[0], down_matrix[0]
    cols = (((1,), (1,)), ((), ()))
    gate_pre = jnp.dot(x, w_gate, preferred_element_type=F32)
    up_pre = jnp.dot(x, w_up, preferred_element_type=F32)
    back = lax.dot_general(y, w_down, cols, preferred_element_type=F32)
    sig = jax.nn.sigmoid(gate_pre)
    act = gate_pre * sig
    hidden = act * up_pre
    gate_grad = (back * up_pre * sig * (1.0 + gate_pre * (1.0 - sig))).astype(BF16)
    up_grad = (back * act).astype(BF16)
    scores = jnp.sum(hidden * back, axis=1)
    line = -(-capacity // 128) * 128
    scores = jnp.pad(scores.reshape(2, experts, 1, capacity), ((0, 0), (0, 0), (0, 0), (0, line - capacity)))
    back_rows, back_scores, norms_all, down_norms, gate_full, up_full, down_full = send_back(
        gate_grad, up_grad, w_gate, w_up, x, hidden.astype(BF16), y, scores, experts, n_tp
    )
    token_gradient = jnp.dot(
        by_token, back_rows.reshape(slots, part), preferred_element_type=F32
    ).astype(BF16)
    pair_scores = back_scores[:, 0, :capacity].reshape(slots)
    mixing_gradient = jnp.sum(jnp.where(matches, pair_scores[None, None, :], 0.0), axis=2) / mixing
    return (
        token_gradient,
        mixing_gradient,
        gate_full[None],
        up_full[None],
        down_full[None],
        norms_all[None],
        down_norms,
    )


def solution(mesh):
    placed = (
        P("ep", "tp"), P("ep", None), P("ep", None), P("ep", None, "tp"),
        P("ep", None, "tp"), P("ep", "tp", None), P("ep", "tp"),
    )
    return jax.shard_map(
        on_device,
        mesh=mesh,
        in_specs=placed,
        out_specs=(
            P("ep", "tp"), P("ep", None), P("ep", None, "tp"), P("ep", None, "tp"),
            P("ep", "tp", None), P("ep", None, None), P("ep", "tp"),
        ),
        check_vma=False,
    )
```

```python
import functools

import jax
import jax.numpy as jnp
from jax import lax
from jax.experimental import pallas as pl
from jax.experimental.pallas import tpu as pltpu
from jax.sharding import PartitionSpec as P

MESH = pl.DeviceIdType.MESH
F32 = jnp.float32
BF16 = jnp.bfloat16


def send(src, dst, send_sem, recv_sem, ep, tp):
    copy = pltpu.make_async_remote_copy(
        src_ref=src, dst_ref=dst, send_sem=send_sem, recv_sem=recv_sem,
        device_id=(ep, tp), device_id_type=MESH,
    )
    copy.start()
    return copy


def arrived(ref, sem):
    pltpu.make_async_copy(ref, ref, sem).wait()


def places():
    ep, tp = lax.axis_index("ep"), lax.axis_index("tp")
    return ep // 2, ep % 2, tp


def tp_peer(tp, step, n_tp):
    if n_tp == 4:
        x, y = tp % 2, tp // 2
        return ((1 - y) if step // 2 else y) * 2 + ((1 - x) if step % 2 else x)
    return (tp + step) % n_tp


def tp_from(tp, step, n_tp):
    if n_tp == 4:
        return tp_peer(tp, step, n_tp)
    return (tp + n_tp - step) % n_tp


def greet(zs, n_tp, z, c, t):
    barrier = pltpu.get_barrier_semaphore()
    for k in range(1, zs):
        pl.semaphore_signal(barrier, inc=1, device_id=((z + k) % zs * 2 + c, t), device_id_type=MESH)
    for k in range(1, n_tp):
        pl.semaphore_signal(barrier, inc=1, device_id=(z * 2 + c, (t + k) % n_tp), device_id_type=MESH)
    pl.semaphore_signal(barrier, inc=1, device_id=(z * 2 + 1 - c, t), device_id_type=MESH)
    pl.semaphore_wait(barrier, zs + n_tp - 1)


def distances(zs):
    order = []
    for k in range(1, zs // 2 + 1):
        order.append(k)
        if zs - k != k:
            order.append(zs - k)
    return order


def dispatch_kernel(
    zs, n_tp, part, x_in, y_in, x_out, y_out, ep_send, ep_recv, tp_send, tp_recv,
    fwd_send, core_send, core_recv,
):
    z, c, t = places()
    chunks = zs if zs <= 4 else 1
    span = zs // chunks
    ins, outs = (x_in, y_in), (x_out, y_out)
    greet(zs, n_tp, z, c, t)

    def block(a, core, q, feat):
        cols = pl.ds(pl.multiple_of(feat * part, part), part)
        return outs[a].at[core, pl.ds(q * span, span), :, cols]

    def mine(a):
        cols = pl.ds(pl.multiple_of(t * part, part), part)
        return outs[a].at[c, z, :, cols]

    sent = []
    home = z // span
    for a in range(2):
        pltpu.make_async_copy(ins[a].at[z], mine(a), ep_recv.at[a, home]).start()
    for k in distances(zs):
        for a in range(2):
            dest = (z + k) % zs
            sent.append(send(ins[a].at[dest], mine(a), ep_send.at[a, k], ep_recv.at[a, home], dest * 2 + c, t))

    direct = (1, 2) if n_tp == 4 else range(1, n_tp)

    def to_core(a, q, feat):
        ref = block(a, c, q, feat)
        sent.append(send(ref, ref, core_send.at[a, q, feat], core_recv.at[a, q, feat], z * 2 + 1 - c, t))

    def spread(q):
        for a in range(2):
            ref = block(a, c, q, t)
            arrived(ref, ep_recv.at[a, q])
            for s in direct:
                sent.append(send(ref, ref, tp_send.at[a, q, s], tp_recv.at[a, q, t], z * 2 + c, tp_peer(t, s, n_tp)))
            to_core(a, q, t)

    def relay(q):
        if n_tp == 4:
            for a, s in ((0, 1), (1, 2), (1, 1), (0, 2)):
                feat = tp_from(t, s, n_tp)
                ref = block(a, c, q, feat)
                arrived(ref, tp_recv.at[a, q, feat])
                if s == a + 1:
                    sent.append(send(ref, ref, fwd_send.at[a, q], tp_recv.at[a, q, feat], z * 2 + c, tp_peer(t, 3 - s, n_tp)))
                to_core(a, q, feat)
        else:
            for s in direct:
                feat = tp_from(t, s, n_tp)
                for a in range(2):
                    arrived(block(a, c, q, feat), tp_recv.at[a, q, feat])
                    to_core(a, q, feat)

    def finish(q):
        if n_tp == 4:
            feat = tp_from(t, 3, n_tp)
            for a in range(2):
                arrived(block(a, c, q, feat), tp_recv.at[a, q, feat])
                to_core(a, q, feat)

    if chunks == 1:
        order = [0]
    else:
        order = [z] + [(z + zs - k) % zs for k in distances(zs)]
    for i in range(chunks + 2):
        if i < chunks:
            spread(order[i])
        if 1 <= i <= chunks:
            relay(order[i - 1])
        if i >= 2:
            finish(order[i - 2])
    for a in range(2):
        for q in range(chunks):
            for feat in range(n_tp):
                arrived(block(a, 1 - c, q, feat), core_recv.at[a, q, feat])
    for copy in sent:
        copy.wait_send()


def dispatch(x, y, zs, n_tp):
    _, cap, part = x.shape
    chunks = zs if zs <= 4 else 1
    out = jax.ShapeDtypeStruct((2, zs, cap, n_tp * part), BF16)
    vm = pl.BlockSpec(memory_space=pltpu.VMEM)
    dma = pltpu.SemaphoreType.DMA
    return pl.pallas_call(
        functools.partial(dispatch_kernel, zs, n_tp, part),
        out_shape=(out, out),
        in_specs=[vm, vm],
        out_specs=(vm, vm),
        scratch_shapes=[
            dma((2, zs)), dma((2, chunks)), dma((2, chunks, n_tp)), dma((2, chunks, n_tp)),
            dma((2, chunks)), dma((2, chunks, n_tp)), dma((2, chunks, n_tp)),
        ],
        compiler_params=pltpu.CompilerParams(collective_id=0, has_side_effects=True, vmem_limit_bytes=48 << 20),
        name="dispatch",
    )(x, y)


def hail(zs, n_tp, z, c, t):
    barrier = pltpu.get_barrier_semaphore()
    for k in range(1, zs):
        pl.semaphore_signal(barrier, inc=1, device_id=((z + k) % zs * 2 + c, t), device_id_type=MESH)
    for k in range(1, n_tp):
        pl.semaphore_signal(barrier, inc=1, device_id=(z * 2 + c, (t + k) % n_tp), device_id_type=MESH)
    pl.semaphore_signal(barrier, inc=1, device_id=(z * 2 + 1 - c, t), device_id_type=MESH)
    return lambda: pl.semaphore_wait(barrier, zs + n_tp - 1)


def lane_sums(square):
    folded = square[:, :128]
    for k in range(1, square.shape[1] // 128):
        folded = folded + square[:, k * 128:(k + 1) * 128]
    return jnp.sum(folded.T, axis=0, keepdims=True)


def return_kernel(
    zs, n_tp, part,
    gate_hbm, up_hbm, w_gate_hbm, w_up_hbm, x_hbm, hidden_hbm, y_hbm, scores,
    out_rows, out_scores, out_norms, out_down_norms, gate_out, up_out, down_out,
    gate_grad, up_grad, w_gate, w_up, x, hidden, y, gate_full, up_full, down_full, norms, folded,
    all_rows, other, other_scores, both, both_scores, pieces, score_pieces, norm_pieces, total, total_scores,
    passing, passed, pass_send, pass_recv, sum_send, sum_recv, load_sem, store_sem,
    core_send, core_recv, cs_send, cs_recv, tp_send, tp_recv, ts_send, ts_recv,
    tn_send, tn_recv, ep_send, ep_recv, es_send, es_recv,
):
    z, c, t = places()
    chunks = zs if zs <= 4 else 1
    span = zs // chunks
    cap = out_rows.shape[1]
    width, hid = w_gate.shape
    half = zs * cap
    everyone_in = hail(zs, n_tp, z, c, t)
    loads = []
    for i, (src, dst) in enumerate((
        (gate_hbm, gate_grad), (up_hbm, up_grad), (w_gate_hbm, w_gate), (w_up_hbm, w_up),
        (x_hbm, x), (hidden_hbm, hidden), (y_hbm, y),
    )):
        copy = pltpu.make_async_copy(src, dst, load_sem.at[i])
        copy.start()
        loads.append(copy)
    stores = []

    def store(i, src, dst):
        copy = pltpu.make_async_copy(src, dst, store_sem.at[i])
        copy.start()
        stores.append(copy)

    across = (((1,), (1,)), ((), ()))
    down = (((0,), (0,)), ((), ()))
    tile = min(256, width)

    def row_terms():
        @pl.loop(0, width // tile)
        def _(j):
            at = pl.ds(pl.multiple_of(j * tile, tile), tile)
            term = (
                lax.dot_general(gate_grad[...].reshape(2 * half, hid), w_gate[at, :], across, preferred_element_type=F32)
                + lax.dot_general(up_grad[...].reshape(2 * half, hid), w_up[at, :], across, preferred_element_type=F32)
            ).astype(BF16)
            all_rows[0, :, at] = term[:half]
            all_rows[1, :, at] = term[half:]

    sent = []
    if chunks == 1:
        order = [0]
    else:
        order = [(z + k) % zs for k in reversed(distances(zs))] + [z]
    mate = z * 2 + 1 - c

    def rows_of(q):
        if chunks == 1:
            return slice(None)
        return pl.ds(pl.multiple_of(q * cap, cap), cap)

    for copy in loads[:4]:
        copy.wait()
    row_terms()
    everyone_in()
    for q in order:
        sent.append(send(all_rows.at[1 - c, rows_of(q)], other.at[rows_of(q)], core_send.at[q], core_recv.at[q], mate, t))
    sent.append(send(scores.at[1 - c], other_scores, cs_send, cs_recv, mate, t))

    def cols(feat):
        return pl.ds(pl.multiple_of(feat * part, part), part)

    def reduce_core(q):
        at = rows_of(q)
        arrived(other.at[at], core_recv.at[q])
        both[at, :] = (all_rows[c, at, :].astype(F32) + other[at, :].astype(F32)).astype(BF16)
        if n_tp == 4:
            far_side = tp_peer(t, 3, n_tp)
            for s in (1, 2):
                sent.append(send(both.at[at, half_cols(far_side, s - 1)], passing.at[s - 1, at], pass_send.at[s - 1, q], pass_recv.at[s - 1, q], z * 2 + c, tp_peer(t, s, n_tp)))
            for s in (1, 2):
                feat = tp_peer(t, s, n_tp)
                sent.append(send(both.at[at, half_cols(feat, s - 1)], piece_half(s, at, s - 1), tp_send.at[s, q], tp_recv.at[s, q], z * 2 + c, feat))
        else:
            for s in reversed(range(1, n_tp)):
                feat = tp_peer(t, s, n_tp)
                sent.append(send(both.at[at, cols(feat)], pieces.at[s, at], tp_send.at[s, q], tp_recv.at[s, q], z * 2 + c, feat))

    def half_cols(feat, u):
        return pl.ds(pl.multiple_of(feat * part + u * (part // 2), part // 2), part // 2)

    def piece_half(s, at, u):
        return pieces.at[s, at, pl.ds(u * (part // 2), part // 2)]

    def pass_on(q):
        if n_tp == 4:
            at = rows_of(q)
            for s in (1, 2):
                u, turn = s - 1, 3 - s
                feat = tp_peer(t, turn, n_tp)
                arrived(passing.at[u, at], pass_recv.at[u, q])
                passed[u, at, :] = (passing[u, at, :].astype(F32) + both[at, half_cols(feat, u)].astype(F32)).astype(BF16)
                sent.append(send(passed.at[u, at], piece_half(turn, at, u), sum_send.at[turn, q], sum_recv.at[turn, q], z * 2 + c, feat))

    for q in order:
        reduce_core(q)
    arrived(other_scores, cs_recv)
    both_scores[...] = scores[c] + other_scores[...]
    for s in range(1, n_tp):
        sent.append(send(both_scores, score_pieces.at[s], ts_send.at[s], ts_recv.at[s], z * 2 + c, tp_peer(t, s, n_tp)))

    def reduce_tp(q):
        at = rows_of(q)
        if n_tp == 4:
            for s in (1, 2):
                arrived(piece_half(s, at, s - 1), tp_recv.at[s, q])
                arrived(piece_half(s, at, 2 - s), sum_recv.at[s, q])
        else:
            for s in reversed(range(1, n_tp)):
                arrived(pieces.at[s, at], tp_recv.at[s, q])
        for j in range(span):
            sub = at if chunks > 1 else slice(j * cap, (j + 1) * cap)
            acc = both[sub, cols(t)].astype(F32)
            for s in (1, 2) if n_tp == 4 else range(1, n_tp):
                acc = acc + pieces[s, sub, :].astype(F32)
            total[q * span + j] = acc.astype(BF16)

    def go_home(dest, k):
        sent.append(send(total.at[dest], out_rows.at[z], ep_send.at[k], ep_recv.at[k], dest * 2 + c, t))

    def input_tiles(first, last):
        @pl.loop(first * tile // g_tile, last * tile // g_tile)
        def _(j):
            at = pl.ds(pl.multiple_of(j * g_tile, g_tile), g_tile)
            columns = x[:, at].T
            for i, (grad, full) in enumerate(((gate_grad, gate_full), (up_grad, up_full))):
                term = jnp.dot(columns, grad[...].reshape(2 * half, hid), preferred_element_type=F32)
                full[at, :] = term.astype(BF16)
                norms[pl.ds(i, 1), at] = lane_sums(term * term)

    h_tile = min(256, hid)
    g_tile = min(512, width)
    wide = min(512, width)

    def down_tiles(i):
        at = slice(i * h_tile, (i + 1) * h_tile)
        folded[...] = jnp.zeros_like(folded)
        turned = hidden[:, at].T

        @pl.loop(0, width // wide)
        def _(j):
            lanes = pl.ds(pl.multiple_of(j * wide, wide), wide)
            term = jnp.dot(turned, y[:, lanes], preferred_element_type=F32)
            down_full[at, lanes] = term.astype(BF16)
            square = term * term
            acc = square[:, :128]
            for k in range(1, wide // 128):
                acc = acc + square[:, k * 128:(k + 1) * 128]
            folded[...] += acc

        out_down_norms[:, at] = jnp.sum(folded[...].T, axis=0, keepdims=True)

    away = list(reversed(distances(zs)))
    n_tiles = width // tile

    def phase_input(first, last):
        if first == 0:
            loads[4].wait()
        input_tiles(first, last)
        if last == n_tiles:
            store(0, gate_full, gate_out)
            store(1, up_full, up_out)
            for s in range(1, n_tp):
                sent.append(send(norms, norm_pieces.at[s], tn_send.at[s], tn_recv.at[s], z * 2 + c, tp_peer(t, s, n_tp)))

    def phase_down(first, last):
        if first == 0:
            loads[5].wait()
            loads[6].wait()
        for i in range(first, last):
            down_tiles(i)
        if last == hid // h_tile:
            store(2, down_full, down_out)

    h_count = hid // h_tile
    phases = [
        lambda: phase_input(0, n_tiles // 2),
        lambda: phase_input(n_tiles // 2, n_tiles),
        lambda: phase_down(0, h_count // 2) if h_count > 1 else None,
        lambda: phase_down(h_count // 2, h_count),
    ]
    if chunks < len(phases):
        for phase in phases:
            phase()
        phases = []
    pass_on(order[0])
    if chunks > 1:
        pass_on(order[1])
    for i in range(chunks):
        if i < len(phases):
            phases[i]()
        if i + 2 < chunks:
            pass_on(order[i + 2])
        reduce_tp(order[i])
        if chunks > 1:
            if i < len(away):
                go_home(order[i], away[i])
        else:
            for k in away:
                go_home((z + k) % zs, k)
        if i == 0:
            for s in range(1, n_tp):
                arrived(score_pieces.at[s], ts_recv.at[s])
            acc = both_scores[...]
            for s in range(1, n_tp):
                acc = acc + score_pieces[s]
            total_scores[...] = acc
            for k in away:
                dest = (z + k) % zs
                sent.append(send(total_scores.at[dest], out_scores.at[z], es_send.at[k], es_recv.at[k], dest * 2 + c, t))
            out_scores[z] = total_scores[z]
    out_rows[z] = total[z]
    acc = norms[...]
    for s in range(1, n_tp):
        arrived(norm_pieces.at[s], tn_recv.at[s])
        acc = acc + norm_pieces[s]
    out_norms[...] = acc
    for k in away:
        src = (z + zs - k) % zs
        arrived(out_scores.at[src], es_recv.at[k])
        arrived(out_rows.at[src], ep_recv.at[k])
    for copy in stores:
        copy.wait()
    for copy in sent:
        copy.wait_send()


def send_back(gate_grad, up_grad, w_gate, w_up, x, hidden, y, scores, zs, n_tp):
    rows, width = x.shape
    hid = hidden.shape[1]
    part, half = width // n_tp, rows // 2
    cap = half // zs
    chunks = zs if zs <= 4 else 1
    vm = pl.BlockSpec(memory_space=pltpu.VMEM)
    far = pl.BlockSpec(memory_space=pltpu.HBM)
    dma = pltpu.SemaphoreType.DMA
    line = scores.shape[2:]
    gradient = jax.ShapeDtypeStruct((width, hid), BF16)
    return pl.pallas_call(
        functools.partial(return_kernel, zs, n_tp, part),
        out_shape=(
            jax.ShapeDtypeStruct((zs, cap, part), BF16),
            jax.ShapeDtypeStruct((zs,) + line, F32),
            jax.ShapeDtypeStruct((2, width), F32),
            jax.ShapeDtypeStruct((1, hid), F32),
            gradient, gradient, jax.ShapeDtypeStruct((hid, width), BF16),
        ),
        in_specs=[far] * 7 + [vm],
        out_specs=(vm,) * 4 + (far,) * 3,
        scratch_shapes=[
            pltpu.VMEM((2, half, hid), BF16), pltpu.VMEM((2, half, hid), BF16),
            pltpu.VMEM((width, hid), BF16), pltpu.VMEM((width, hid), BF16),
            pltpu.VMEM((rows, width), BF16), pltpu.VMEM((rows, hid), BF16), pltpu.VMEM((rows, width), BF16),
            pltpu.VMEM((width, hid), BF16), pltpu.VMEM((width, hid), BF16), pltpu.VMEM((hid, width), BF16),
            pltpu.VMEM((2, width), F32), pltpu.VMEM((min(256, hid), 128), F32),
            pltpu.VMEM((2, half, width), BF16), pltpu.VMEM((half, width), BF16),
            pltpu.VMEM((zs,) + line, F32),
            pltpu.VMEM((half, width), BF16),
            pltpu.VMEM((zs,) + line, F32),
            pltpu.VMEM((n_tp, half, part), BF16),
            pltpu.VMEM((n_tp, zs) + line, F32),
            pltpu.VMEM((n_tp, 2, width), F32),
            pltpu.VMEM((zs, cap, part), BF16),
            pltpu.VMEM((zs,) + line, F32),
            pltpu.VMEM((2, half, part // 2), BF16), pltpu.VMEM((2, half, part // 2), BF16),
            dma((2, chunks)), dma((2, chunks)), dma((3, chunks)), dma((3, chunks)),
            dma((7,)), dma((3,)),
            dma((chunks,)), dma((chunks,)), dma, dma,
            dma((n_tp, chunks)), dma((n_tp, chunks)), dma((n_tp,)), dma((n_tp,)),
            dma((n_tp,)), dma((n_tp,)), dma((zs,)), dma((zs,)), dma((zs,)), dma((zs,)),
        ],
        compiler_params=pltpu.CompilerParams(collective_id=1, has_side_effects=True, vmem_limit_bytes=50 << 20),
        name="send_back",
    )(gate_grad.reshape(2, half, hid), up_grad.reshape(2, half, hid), w_gate, w_up, x, hidden, y, scores)


def fused_kernel(
    zs, n_tp, part, cap, tok,
    routing_hbm, mixing_hbm, tokens_hbm, upstream_hbm, w_gate_hbm, w_up_hbm, w_down_hbm,
    out_tokens, out_mixing, out_norms, out_down_norms, gate_full, up_full, down_full,
    routing, mixing, tokens, upstream, w_gate, w_up, w_down, gate_turned, up_turned, down_turned,
    x_put, y_put, x_all, y_all, gate_grad, up_grad, hidden, targets,
    all_rows, other, both, passing, passed, pieces, total, back_rows,
    scores, other_scores, both_scores, score_pieces, total_scores, back_scores,
    norms, norm_pieces,
    folded, hidden_turned, load_sem, own_sem, ep_send, ep_recv, tp_send, tp_recv, fwd_send, core_send, core_recv,
    swap_send, swap_recv, ring_send, pass_recv, sum_recv,
    cs_send, cs_recv, ts_send, ts_recv, tn_send, tn_recv, home_send, home_recv, es_send, es_recv,
):
    z, c, t = places()
    here, mate = z * 2 + c, z * 2 + 1 - c
    peers = [tp_peer(t, s, n_tp) for s in range(n_tp)]
    width, hid = w_gate.shape
    rows = 2 * cap
    loads = []
    for i, (src, dst) in enumerate((
        (routing_hbm, routing), (mixing_hbm, mixing), (tokens_hbm, tokens), (upstream_hbm, upstream),
        (w_down_hbm, w_down), (w_gate_hbm, w_gate), (w_up_hbm, w_up),
    )):
        copy = pltpu.make_async_copy(src, dst, load_sem.at[i])
        copy.start()
        loads.append(copy)
    everyone_in = hail(zs, n_tp, z, c, t)
    across = (((1,), (1,)), ((), ()))
    first = (((0,), (0,)), ((), ()))
    def push(src, dst, send_sem, recv_sem, ep, tp):
        send(src, dst, send_sem, recv_sem, ep, tp)

    def cols(feat):
        return pl.ds(pl.multiple_of(feat * part, part), part)

    def half_cols(feat, u):
        return pl.ds(pl.multiple_of(feat * part + u * (part // 2), part // 2), part // 2)

    lanes = -(-zs // 16) * 16
    experts_at = lax.broadcasted_iota(jnp.int32, (lanes, tok), 0)
    before = lax.broadcasted_iota(jnp.int32, (tok, tok), 0) < lax.broadcasted_iota(jnp.int32, (tok, tok), 1)
    for copy in loads[:2]:
        copy.wait()
    picks = [routing[k:k + 1, :] == experts_at for k in range(routing.shape[0])]
    chosen = sum(pick.astype(F32) for pick in picks)
    earlier = jnp.dot(chosen.astype(BF16), before.astype(F32).astype(BF16), preferred_element_type=F32)
    for k, pick in enumerate(picks):
        place = jnp.sum(jnp.where(pick, earlier, 0.0), axis=0, keepdims=True)
        targets[k:k + 1, :] = routing[k:k + 1, :] * cap + place.astype(jnp.int32)

    def matches(e):
        slots_at = lax.broadcasted_iota(jnp.int32, (cap, tok), 0) + e * cap
        return [targets[k:k + 1, :] == slots_at for k in range(len(picks))]

    for copy in loads[2:4]:
        copy.wait()
    for e in range(zs):
        hits = matches(e)
        pick = sum(hit.astype(F32) for hit in hits).astype(BF16)
        weight = sum(jnp.where(hit, mixing[k:k + 1, :], 0.0) for k, hit in enumerate(hits))
        x_put[e] = jnp.dot(pick, tokens[...], preferred_element_type=F32).astype(BF16)
        placed = jnp.dot(pick, upstream[...], preferred_element_type=F32)
        y_put[e] = (placed * jnp.sum(weight, axis=1, keepdims=True)).astype(BF16)
    scores[...] = jnp.zeros_like(scores)
    everyone_in()

    outer = (z - 1) * (z - 2) // 2
    order = [z, 1 + z % 2, 3 - 3 * (z % 2), (z + 2) % zs]
    lands = [0, 1 + outer, 1 + outer, 3]
    puts, alls = (x_put, y_put), (x_all, y_all)

    def block(a, i, core, feat):
        return alls[a].at[i, core, :, cols(feat)]

    def slab(a, i, feat, u):
        return alls[a].at[i, c, :, half_cols(feat, u)]

    for a in range(2):
        copy = pltpu.make_async_copy(puts[a].at[z], block(a, 0, c, t), own_sem)
        copy.start()

    def over(i):
        return [
            pltpu.make_async_remote_copy(
                src_ref=puts[a].at[order[i]], dst_ref=block(a, lands[i], c, t), send_sem=ep_send,
                recv_sem=ep_recv.at[a, lands[i]], device_id=(order[i] * 2 + c, t), device_id_type=MESH,
            )
            for a in range(2)
        ]

    def cross(i):
        for copy in over(i):
            copy.start()

    def to_core(a, i, feat, src=None):
        ref = block(a, i, c, feat)
        push(ref if src is None else src, ref, core_send, core_recv.at[i], mate, t)

    def spread(i, apart=False):
        halves = [pl.ds(u * (part // 2), part // 2) for u in range(2)]

        def land(a):
            if i:
                arrived(block(a, i, c, t), ep_recv.at[a, i])

        def near(a):
            for u in range(2):
                ref = slab(a, i, t, u)
                push(ref if i else puts[a].at[z, :, halves[u]], ref, tp_send, tp_recv.at[i, 2 * a + u], here, peers[1 + a])

        def other_way(a):
            ref = block(a, i, c, t)
            push(ref if i else puts[a].at[z], ref, tp_send, tp_recv.at[i, 4], here, peers[2 - a])

        def over_core(a):
            to_core(a, i, t, None if i else puts[a].at[z])

        if apart:
            for a in range(2):
                land(a)
                near(a)
                other_way(a)
                over_core(a)
        else:
            for step in (land, near, other_way, over_core):
                for a in range(2):
                    step(a)

    def relay(i):
        for u in range(2):
            for a in range(2):
                ref = slab(a, i, peers[1 + a], u)
                arrived(ref, tp_recv.at[i, 2 * a + u])
                push(ref, ref, fwd_send, tp_recv.at[i, 5], here, peers[2 - a])
        for a in range(2):
            to_core(a, i, peers[1 + a])

    def pair_of(i):
        return x_all.at[i, :, :, pl.ds(0, part)]

    def finish(i):
        arrived(pair_of(i), tp_recv.at[i, 4])
        for a in range(2):
            to_core(a, i, peers[2 - a])
        arrived(pair_of(i), tp_recv.at[i, 5])
        for a in range(2):
            to_core(a, i, peers[3])

    square = min(256, hid)
    eye = (
        lax.broadcasted_iota(jnp.int32, (square, square), 0) == lax.broadcasted_iota(jnp.int32, (square, square), 1)
    ).astype(F32).astype(BF16)

    def turn_down():
        loads[4].wait()

        @pl.loop(0, width // square, unroll=4)
        def _(j):
            at = pl.ds(pl.multiple_of(j * square, square), square)
            down_turned[at, :] = lax.dot_general(eye, w_down[:, at], across, preferred_element_type=F32).astype(BF16)

    def turn_in(a):
        loads[5 + a].wait()
        src, dst = ((w_gate, gate_turned), (w_up, up_turned))[a]

        @pl.loop(0, width // square, unroll=4)
        def _(j):
            at = pl.ds(pl.multiple_of(j * square, square), square)
            for h in range(hid // square):
                lines = slice(h * square, (h + 1) * square)
                dst[lines, at] = lax.dot_general(eye, src[at, lines], across, preferred_element_type=F32).astype(BF16)

    h_tile = min(256, hid)

    def forward(i):
        if i == 0:
            arrived(pair_of(0), own_sem)
        arrived(x_all.at[i], core_recv.at[i])
        for j in range(hid // h_tile):
            at = slice(j * h_tile, (j + 1) * h_tile)
            gate_pre = jnp.dot(x_all[i].reshape(rows, width), w_gate[:, at], preferred_element_type=F32)
            up_pre = jnp.dot(x_all[i].reshape(rows, width), w_up[:, at], preferred_element_type=F32)
            back = jnp.dot(y_all[i].reshape(rows, width), down_turned[:, at], preferred_element_type=F32)
            sig = jax.nn.sigmoid(gate_pre)
            act = gate_pre * sig
            low = act * up_pre
            gate_grad[i, :, :, at] = (back * up_pre * sig * (1.0 + gate_pre * (1.0 - sig))).astype(BF16).reshape(2, cap, h_tile)
            up_grad[i, :, :, at] = (back * act).astype(BF16).reshape(2, cap, h_tile)
            hidden[i, :, :, at] = low.astype(BF16).reshape(2, cap, h_tile)
            terms = low * back
            for core in range(2):
                scores[core, i, :, :cap] += lane_sums(terms[core * cap:(core + 1) * cap])

    def row_terms(i, steps=(3, 1, 2, 0)):
        for s in steps:
            at = cols(peers[s])
            term = (
                jnp.dot(gate_grad[i].reshape(rows, hid), gate_turned[:, at], preferred_element_type=F32)
                + jnp.dot(up_grad[i].reshape(rows, hid), up_turned[:, at], preferred_element_type=F32)
            ).astype(BF16)
            all_rows[i, :, :, at] = term.reshape(2, cap, part)
            push(all_rows.at[i, 1 - c, :, at], other.at[i, :, at], swap_send, swap_recv.at[i, 0 if s == 3 else 1], mate, t)

    def piece_half(s, i, u):
        return pieces.at[s - 1, i, :, pl.ds(u * (part // 2), part // 2)]

    def reduce_core(i, steps=(3, 1, 2, 0)):
        for s in steps:
            at = cols(peers[s])
            if s == 3:
                arrived(other.at[i, :, at], swap_recv.at[i, 0])
            elif s == 1:
                arrived(other.at[i, :, pl.ds(0, (n_tp - 1) * part)], swap_recv.at[i, 1])
            both[i, :, at] = (all_rows[i, c, :, at].astype(F32) + other[i, :, at].astype(F32)).astype(BF16)
            if s == 3:
                for u in range(2):
                    push(both.at[i, :, half_cols(peers[3], u)], passing.at[u, i], ring_send, pass_recv.at[i], here, peers[u + 1])
            elif s:
                u = s - 1
                push(both.at[i, :, half_cols(peers[s], u)], piece_half(s, i, u), ring_send, sum_recv.at[i], here, peers[s])

    def pass_on(i):
        arrived(passing.at[:, i], pass_recv.at[i])
        for u in range(2):
            turn = 2 - u
            passed[u, i] = (passing[u, i].astype(F32) + both[i, :, half_cols(peers[turn], u)].astype(F32)).astype(BF16)
            push(passed.at[u, i], piece_half(turn, i, u), ring_send, sum_recv.at[i], here, peers[turn])

    def reduce_tp(i):
        arrived(pieces.at[:, i], sum_recv.at[i])
        acc = both[i, :, cols(t)].astype(F32) + pieces[0, i].astype(F32) + pieces[1, i].astype(F32)
        if i == 0:
            back_rows[z] = acc.astype(BF16)
        else:
            total[i] = acc.astype(BF16)
            push(total.at[i], back_rows.at[z], home_send, home_recv.at[z], order[i] * 2 + c, t)

    g_tile = min(512, width)

    def input_tiles(begin, end):
        @pl.loop(begin, end, unroll=min(2, end - begin))
        def _(j):
            at = pl.ds(pl.multiple_of(j * g_tile, g_tile), g_tile)
            columns = x_all[:, :, :, at].reshape(zs * rows, g_tile).T
            for i, (grad, full) in enumerate(((gate_grad, gate_full), (up_grad, up_full))):
                term = jnp.dot(columns, grad[...].reshape(zs * rows, hid), preferred_element_type=F32)
                full[at, :] = term.astype(BF16)
                norms[pl.ds(i, 1), at] = lane_sums(term * term)

    def turn_hidden():
        hidden_turned[...] = hidden[...].reshape(zs * rows, hid).T

    def down_tiles(begin, end):
        if begin == 0:
            folded[...] = jnp.zeros_like(folded)

        @pl.loop(begin, end, unroll=min(2, end - begin))
        def _(j):
            at = pl.ds(pl.multiple_of(j * g_tile, g_tile), g_tile)
            term = jnp.dot(hidden_turned[...], y_all[:, :, :, at].reshape(zs * rows, g_tile), preferred_element_type=F32)
            down_full[:, at] = term.astype(BF16)
            term = term * term
            acc = term[:, :128]
            for k in range(1, g_tile // 128):
                acc = acc + term[:, k * 128:(k + 1) * 128]
            folded[...] += acc

        if end == n_in:
            out_down_norms[...] = jnp.sum(folded[...].T, axis=0, keepdims=True)

    def send_norms():
        for s in range(1, n_tp):
            push(norms, norm_pieces.at[s], tn_send, tn_recv, here, peers[s])

    def swap_scores():
        push(scores.at[1 - c], other_scores, cs_send, cs_recv, mate, t)

    def spread_scores():
        arrived(other_scores, cs_recv)
        both_scores[...] = scores[c] + other_scores[...]
        for s in range(1, n_tp):
            push(both_scores, score_pieces.at[s], ts_send, ts_recv, here, peers[s])

    def home_scores():
        acc = both_scores[...]
        arrived(score_pieces.at[pl.ds(1, n_tp - 1)], ts_recv)
        for s in range(1, n_tp):
            acc = acc + score_pieces[s]
        total_scores[...] = acc
        for i in range(1, zs):
            push(total_scores.at[i], back_scores.at[z], es_send, es_recv, order[i] * 2 + c, t)
        back_scores[z] = total_scores[0]

    def close_norms():
        acc = norms[...]
        arrived(norm_pieces.at[pl.ds(1, n_tp - 1)], tn_recv)
        for s in range(1, n_tp):
            acc = acc + norm_pieces[s]
        out_norms[...] = acc

    def close_scores():
        arrived(back_scores.at[pl.ds(0, zs - 1)], es_recv)
        for k in range(len(picks)):
            found = jnp.zeros((1, tok), F32)
            for e in range(zs):
                column = jnp.broadcast_to(back_scores[e], (8, back_scores.shape[2])).T[:cap, :1]
                found = found + jnp.sum(jnp.where(matches(e)[k], column, 0.0), axis=0, keepdims=True)
            out_mixing[k:k + 1, :] = found / mixing[k:k + 1, :]

    def close_tokens():
        last = (z + 2) % zs
        acc = jnp.zeros((tok, part), F32)
        for k in range(1, zs + 1):
            e = (last + k) % zs

            @pl.when(e != z)
            def _():
                arrived(back_rows.at[e], home_recv.at[e])

            pick = sum(hit.astype(F32) for hit in matches(e)).astype(BF16)
            acc = acc + lax.dot_general(pick, back_rows[e], first, preferred_element_type=F32)
        out_tokens[...] = acc.astype(BF16)

    n_in = width // g_tile
    cross(1)
    cross(2)

    @pl.when(outer == 1)
    def _():
        cross(3)

    spread(0)
    turn_down()
    relay(0)
    turn_in(0)
    spread(1)
    turn_in(1)
    finish(0)

    @pl.when(outer == 0)
    def _():
        cross(3)

    relay(1)
    forward(0)
    spread(2)
    row_terms(0)
    finish(1)
    forward(1)
    relay(2)
    spread(3)
    row_terms(1)
    finish(2)
    relay(3)
    reduce_core(1)
    forward(2)
    row_terms(2)
    finish(3)
    reduce_core(2)
    pass_on(1)
    forward(3)
    swap_scores()
    row_terms(3, (3, 1))
    pass_on(2)
    row_terms(3, (2,))
    reduce_core(3, (3,))
    row_terms(3, (0,))
    spread_scores()
    turn_hidden()
    reduce_core(3, (1, 2, 0))
    reduce_tp(1)
    input_tiles(0, 1)
    pass_on(3)
    reduce_tp(2)
    reduce_core(0)
    input_tiles(1, n_in - 1)
    home_scores()
    reduce_tp(3)
    input_tiles(n_in - 1, n_in)
    send_norms()
    pass_on(0)
    down_tiles(0, n_in // 2)
    down_tiles(n_in // 2, n_in)
    reduce_tp(0)
    close_scores()
    close_norms()
    close_tokens()
    arrived(x_all.at[pl.ds(0, zs - 1), :, :, pl.ds(0, part)], ep_send)
    arrived(x_all, core_send)
    arrived(x_all.at[:, :, :, pl.ds(0, 2 * part)], tp_send)
    arrived(x_all.at[:, :, :, pl.ds(0, part)], fwd_send)
    arrived(other, swap_send)
    arrived(x_all.at[pl.ds(0, 3), :, :, pl.ds(0, zs * part // 2)], ring_send)
    arrived(total.at[pl.ds(0, zs - 1)], home_send)
    arrived(other_scores, cs_send)
    arrived(score_pieces.at[pl.ds(0, n_tp - 1)], ts_send)
    arrived(norm_pieces.at[pl.ds(0, n_tp - 1)], tn_send)
    arrived(total_scores.at[pl.ds(0, zs - 1)], es_send)


def settle_kernel(slices, *refs):
    count = len(refs) // 2
    sem = refs[-1]
    copies = []
    for i in range(count):
        lines = refs[i].shape[0]
        parts = slices if lines % (16 * slices) == 0 else 1
        for k in range(parts):
            at = pl.ds(k * (lines // parts), lines // parts)
            copies.append(pltpu.make_async_copy(refs[i].at[at], refs[count + i].at[at], sem.at[i, k]))
    for copy in copies:
        copy.start()
    for copy in copies:
        copy.wait()


def settle(arrays, slices=1):
    far = pl.BlockSpec(memory_space=pltpu.HBM)
    vm = pl.BlockSpec(memory_space=pltpu.VMEM)
    return pl.pallas_call(
        functools.partial(settle_kernel, slices),
        out_shape=tuple(jax.ShapeDtypeStruct(a.shape, a.dtype) for a in arrays),
        in_specs=[vm] * len(arrays),
        out_specs=(far,) * len(arrays),
        scratch_shapes=[pltpu.SemaphoreType.DMA((len(arrays), slices))],
        compiler_params=pltpu.CompilerParams(vmem_limit_bytes=2 << 20),
        name="settle",
    )(*[pltpu.with_memory_space_constraint(a, pltpu.VMEM) for a in arrays])


def fused(routing, mixing, tokens, upstream, w_gate, w_up, w_down, zs, n_tp, cap):
    top, tok = routing.shape
    part = tokens.shape[1]
    width, hid = w_gate.shape
    vm = pl.BlockSpec(memory_space=pltpu.VMEM)
    far = pl.BlockSpec(memory_space=pltpu.HBM)
    dma = pltpu.SemaphoreType.DMA
    line = -(-cap // 128) * 128

    def room(*shape, kind=BF16):
        return pltpu.VMEM(shape, kind)

    return pl.pallas_call(
        functools.partial(fused_kernel, zs, n_tp, part, cap, tok),
        out_shape=(
            room(tok, part), room(top, tok, kind=F32), room(2, width, kind=F32), room(1, hid, kind=F32),
            room(width, hid), room(width, hid), room(hid, width),
        ),
        in_specs=[far] * 7,
        out_specs=(vm,) * 7,
        scratch_shapes=[
            room(top, tok, kind=jnp.int32), room(top, tok, kind=F32), room(tok, part), room(tok, part),
            room(width, hid), room(width, hid), room(hid, width), room(hid, width), room(hid, width), room(width, hid),
            room(zs, cap, part), room(zs, cap, part), room(zs, 2, cap, width), room(zs, 2, cap, width),
            room(zs, 2, cap, hid), room(zs, 2, cap, hid), room(zs, 2, cap, hid), room(top, tok, kind=jnp.int32),
            room(zs, 2, cap, width), room(zs, cap, width), room(zs, cap, width),
            room(2, zs, cap, part // 2), room(2, zs, cap, part // 2), room(2, zs, cap, part),
            room(zs, cap, part), room(zs, cap, part),
            room(2, zs, 1, line, kind=F32), room(zs, 1, line, kind=F32), room(zs, 1, line, kind=F32),
            room(n_tp, zs, 1, line, kind=F32), room(zs, 1, line, kind=F32), room(zs, 1, line, kind=F32),
            room(2, width, kind=F32), room(n_tp, 2, width, kind=F32), room(hid, 128, kind=F32), room(hid, 2 * zs * cap),
            dma((7,)), dma, dma, dma((2, zs)), dma, dma((zs, 6)), dma, dma, dma((zs,)),
            dma, dma((zs, 2)), dma, dma((zs,)), dma((zs,)),
            dma, dma, dma, dma, dma, dma, dma, dma((zs,)), dma, dma,
        ],
        compiler_params=pltpu.CompilerParams(collective_id=2, has_side_effects=True, vmem_limit_bytes=50 << 20),
        name="fused",
    )(*[pltpu.with_memory_space_constraint(a, pltpu.HBM) for a in (routing, mixing, tokens, upstream, w_gate, w_up, w_down)])


def on_device(tokens, routing, mixing, gate_matrix, up_matrix, down_matrix, upstream):
    experts = lax.axis_size("ep") // 2
    n_tp = lax.axis_size("tp")
    tok_rows, part = tokens.shape
    top = routing.shape[1]
    capacity = 5 * top * tok_rows // (4 * experts)
    if experts == 4 and n_tp == 4 and capacity % 16 == 0 and capacity <= 128:
        results = fused(
            routing.T, mixing.T, tokens, upstream, gate_matrix[0], up_matrix[0], down_matrix[0],
            experts, n_tp, capacity,
        )
        grads, mixing_grad, norms_all, down_norms, gate_full, up_full, down_full = settle(results)
        return (
            grads, mixing_grad.T, gate_full[None], up_full[None], down_full[None], norms_all[None], down_norms,
        )
    slots = experts * capacity
    flat = routing.reshape(-1)
    choose = (flat[:, None] == jnp.arange(experts, dtype=jnp.int32)[None, :]).astype(BF16)
    pairs = top * tok_rows
    before = (jnp.arange(pairs)[:, None] > jnp.arange(pairs)[None, :]).astype(BF16)
    earlier = jnp.dot(before, choose, preferred_element_type=F32)
    target = flat * capacity + jnp.sum(earlier * choose.astype(F32), axis=1).astype(jnp.int32)
    spot = target.reshape(tok_rows, top)
    matches = (spot[:, :, None] == jnp.arange(slots, dtype=jnp.int32)[None, None, :])
    by_token = jnp.any(matches, axis=1).astype(BF16)
    scaled = (mixing[:, :, None] * upstream[:, None, :].astype(F32)).astype(BF16)
    rows_first = (((0,), (0,)), ((), ()))
    placed_x = lax.dot_general(by_token, tokens, rows_first, preferred_element_type=F32).astype(BF16)
    placed_y = lax.dot_general(
        matches.reshape(pairs, slots).astype(BF16), scaled.reshape(pairs, part), rows_first,
        preferred_element_type=F32,
    ).astype(BF16)
    x_all, y_all = dispatch(
        placed_x.reshape(experts, capacity, part), placed_y.reshape(experts, capacity, part), experts, n_tp
    )
    width = n_tp * part
    row_count = 2 * slots
    x = x_all.reshape(row_count, width)
    y = y_all.reshape(row_count, width)
    w_gate, w_up, w_down = gate_matrix[0], up_matrix[0], down_matrix[0]
    cols = (((1,), (1,)), ((), ()))
    gate_pre = jnp.dot(x, w_gate, preferred_element_type=F32)
    up_pre = jnp.dot(x, w_up, preferred_element_type=F32)
    back = lax.dot_general(y, w_down, cols, preferred_element_type=F32)
    sig = jax.nn.sigmoid(gate_pre)
    act = gate_pre * sig
    hidden = act * up_pre
    gate_grad = (back * up_pre * sig * (1.0 + gate_pre * (1.0 - sig))).astype(BF16)
    up_grad = (back * act).astype(BF16)
    scores = jnp.sum(hidden * back, axis=1)
    line = -(-capacity // 128) * 128
    scores = jnp.pad(scores.reshape(2, experts, 1, capacity), ((0, 0), (0, 0), (0, 0), (0, line - capacity)))
    back_rows, back_scores, norms_all, down_norms, gate_full, up_full, down_full = send_back(
        gate_grad, up_grad, w_gate, w_up, x, hidden.astype(BF16), y, scores, experts, n_tp
    )
    token_gradient = jnp.dot(
        by_token, back_rows.reshape(slots, part), preferred_element_type=F32
    ).astype(BF16)
    pair_scores = back_scores[:, 0, :capacity].reshape(slots)
    mixing_gradient = jnp.sum(jnp.where(matches, pair_scores[None, None, :], 0.0), axis=2) / mixing
    return (
        token_gradient,
        mixing_gradient,
        gate_full[None],
        up_full[None],
        down_full[None],
        norms_all[None],
        down_norms,
    )


def solution(mesh):
    placed = (
        P("ep", "tp"), P("ep", None), P("ep", None), P("ep", None, "tp"),
        P("ep", None, "tp"), P("ep", "tp", None), P("ep", "tp"),
    )
    return jax.shard_map(
        on_device,
        mesh=mesh,
        in_specs=placed,
        out_specs=(
            P("ep", "tp"), P("ep", None), P("ep", None, "tp"), P("ep", None, "tp"),
            P("ep", "tp", None), P("ep", None, None), P("ep", "tp"),
        ),
        check_vma=False,
    )
```
